32 devices in a mesh: sp: 8 (over z, y), tp: 4 (over x, core).
Axes of the slice: x: 2, y: 2, z: 4, core: 2. Of those that a mesh axis runs over, the one named last changes fastest.
Arguments:
- query_first: bfloat16 [6144, 8, 128], P('sp', 'tp'), may hold values from -5.375 to 5.375
- key_first: bfloat16 [6144, 8, 128], P('sp', 'tp'), may hold values from -5.375 to 5.375
- value_first: bfloat16 [6144, 8, 128], P('sp', 'tp'), may hold values from -6 to 6
- query_second: bfloat16 [6144, 8, 256], P('sp', 'tp'), may hold values from -5.375 to 5.375
- key_second: bfloat16 [6144, 8, 256], P('sp', 'tp'), may hold values from -5.375 to 5.375
- value_second: bfloat16 [6144, 8, 128], P('sp', 'tp'), may hold values from -6 to 6
- mix_lambda: float32 [2, 8], P(None, 'tp'), may hold values from 0.3 to 0.8
- head_gain: float32 [2, 8, 128], P(None, 'tp'), may hold values from 0.1 to 1.9
- out_weight: bfloat16 [2, 8, 128, 2048], P(None, 'tp'), may hold values from -0.125 to 0.125
- residual: bfloat16 [6144, 2048], P(('sp', 'tp')), may hold values from -6 to 6
- norm_gain: float32 [2, 2048], replicated, may hold values from 0.1 to 1.9
- up_weight: bfloat16 [2048, 8192], P('sp', 'tp'), may hold values from -0.125 to 0.125
- down_weight: bfloat16 [8192, 2048], P('tp', 'sp'), may hold values from -0.0625 to 0.0625
Outputs:
- mixed: bfloat16 [6144, 2048], P(('sp', 'tp'))
The draws below stay inside these ranges and needn't reach their ends.
All inputs are finite; a program needn't handle non-finite values.
Results may differ from the reference program's by a relative error of at most 0.02.
Values may be sent and summed in bfloat16 or wider, within the bound.
A program may use at most 128 MiB of HBM per device.

```python
import math
import jax
import jax.numpy as jnp
from jax import lax

D = 2048
FF = 8192
HEADS = 8
KA = 64
KB = 128
VD = 128
TOK_DEV = 768
TOKENS = 6144
N_SP = 8


def drawn_pair(key, group_tag, key_size):
    seeded = jax.random.fold_in(key, group_tag)
    seed_query, seed_keys = jax.random.split(seeded, 2)
    array_shape = (TOKENS, HEADS, 2 * key_size)
    queries = 1.3 * jax.random.truncated_normal(seed_query, -3.4, 3.4, array_shape, jnp.float32)
    key_rows = 1.3 * jax.random.truncated_normal(seed_keys, -3.4, 3.4, array_shape, jnp.float32)
    return (queries, key_rows)


def draw_query_first(key, part):
    return drawn_pair(key, 11, KA)[0].astype(jnp.bfloat16)


def draw_key_first(key, part):
    return drawn_pair(key, 11, KA)[1].astype(jnp.bfloat16)


def draw_query_second(key, part):
    return drawn_pair(key, 23, KB)[0].astype(jnp.bfloat16)


def draw_key_second(key, part):
    return drawn_pair(key, 23, KB)[1].astype(jnp.bfloat16)


def shard_levels(own_key, dims, cuts, smallest, high):
    def one(position, blocks):
        heights = jax.random.uniform(jax.random.fold_in(jax.random.fold_in(own_key, 6), position), (blocks,), jnp.float32, smallest / len(cuts), high / len(cuts))
        return jnp.repeat(jnp.exp(heights), dims[position] // blocks).reshape((-1,) + (1,) * (len(dims) - position - 1))

    loudness = one(*cuts[0])
    for cut in cuts[1:]:
        loudness = loudness * one(*cut)
    return loudness


def scatter_about(key, shape, deviation, limit, cuts=(), kind=jnp.bfloat16):
    drawn = deviation * jax.random.normal(key, shape, jnp.float32)
    if cuts:
        drawn = drawn * shard_levels(key, shape, cuts, -0.22, 0.18)
    return jnp.clip(drawn, -limit, limit).astype(kind)


def setup_inputs(seed: int = 0) -> dict:
    seeds = jax.random.split(jax.random.key(seed), 14)
    return {
        "query_first": draw_query_first(jax.random.fold_in(seeds[13], 71), 0),
        "key_first": draw_key_first(jax.random.fold_in(seeds[13], 71), 0),
        "value_first": scatter_about(seeds[2], (TOKENS, HEADS, VD), 1.0, 6.0, ((0, 8), (1, 4))),
        "query_second": draw_query_second(jax.random.fold_in(seeds[13], 71), 0),
        "key_second": draw_key_second(jax.random.fold_in(seeds[13], 71), 0),
        "value_second": scatter_about(seeds[5], (TOKENS, HEADS, VD), 1.0, 6.0, ((0, 8), (1, 4))),
        "mix_lambda": jnp.clip(0.3 + 0.5 * jax.random.uniform(seeds[6], (2, HEADS), jnp.float32) ** shard_levels(seeds[6], (2, HEADS), ((1, 4),), -0.2, 0.2), 0.3, 0.8),
        "head_gain": jnp.clip(1.0 + 0.18 * jax.random.normal(seeds[7], (2, HEADS, VD), jnp.float32), 0.1, 1.9),
        "out_weight": scatter_about(seeds[8], (2, HEADS, VD, D), D ** -0.5, 0.125, ((1, 4),)),
        "residual": scatter_about(seeds[9], (TOKENS, D), 1.0, 6.0, ((0, 32),)),
        "norm_gain": jnp.clip(1.0 + 0.18 * jax.random.normal(seeds[10], (2, D), jnp.float32), 0.1, 1.9),
        "up_weight": scatter_about(seeds[11], (D, FF), D ** -0.5, 0.125, ((0, 8), (1, 4))),
        "down_weight": scatter_about(seeds[12], (FF, D), FF ** -0.5, 0.0625, ((0, 4), (1, 8))),
    }


EPSILON = 1e-05

def layer_norm(activations, scales):
    average = lax.optimization_barrier(jnp.mean(activations, axis=-1, keepdims=True))
    centred = activations - average
    spread = lax.optimization_barrier(jnp.mean(centred * centred, axis=-1, keepdims=True))
    return centred * lax.rsqrt(spread + EPSILON) * scales

def group_attention(queries_in, keys_in, values_in, lambdas, gains, key_size):
    score_scale = 1.0 / math.sqrt(key_size)
    queries = queries_in.astype(jnp.float32).reshape(TOKENS, HEADS, 2, key_size)
    key_rows = keys_in.astype(jnp.float32).reshape(TOKENS, HEADS, 2, key_size)
    value_rows = values_in.astype(jnp.float32)
    query_blocks = queries.reshape(N_SP, TOK_DEV, HEADS, 2, key_size)

    def one_block(query_block):
        scores = jnp.einsum('qhck,phck->hcqp', query_block, key_rows) * score_scale
        peak = lax.optimization_barrier(jnp.max(scores, axis=-1, keepdims=True))
        exponent = jnp.exp(scores - peak)
        denominator = lax.optimization_barrier(jnp.sum(exponent, axis=-1))
        rounded = lax.optimization_barrier(exponent.astype(jnp.bfloat16)).astype(jnp.float32)
        numerator = jnp.einsum('hcqp,phv->hcqv', rounded, value_rows)
        attended = numerator[:, 0] / denominator[:, 0, :, None] - lambdas[:, None, None] * numerator[:, 1] / denominator[:, 1, :, None]
        mean_square = lax.optimization_barrier(jnp.mean(attended * attended, axis=-1, keepdims=True))
        return (attended * lax.rsqrt(mean_square + EPSILON) * gains[:, None, :]).astype(jnp.bfloat16)
    blocks_out = lax.map(one_block, query_blocks)
    return blocks_out.transpose(1, 0, 2, 3).reshape(HEADS, TOKENS, VD)

def reference(query_first, key_first, value_first, query_second, key_second, value_second, mix_lambda, head_gain, out_weight, residual, norm_gain, up_weight, down_weight):
    heads_first = group_attention(query_first, key_first, value_first, mix_lambda[0], head_gain[0], KA)
    heads_second = group_attention(query_second, key_second, value_second, mix_lambda[1], head_gain[1], KB)
    stacked = jnp.stack([heads_first, heads_second]).astype(jnp.float32)
    projected = jnp.einsum('ghtv,ghvd->td', stacked, out_weight.astype(jnp.float32)) + residual.astype(jnp.float32)
    normed = layer_norm(projected, norm_gain[0])
    expanded = jnp.dot(normed.astype(jnp.bfloat16), up_weight, preferred_element_type=jnp.float32)
    hidden = jnp.square(jnp.maximum(expanded, 0.0)).astype(jnp.bfloat16)
    mixed_sum = jnp.dot(hidden, down_weight, preferred_element_type=jnp.float32)
    return layer_norm(normed + mixed_sum, norm_gain[1]).astype(jnp.bfloat16)
```

```python
import functools
import math

import jax
import jax.numpy as jnp
from jax import lax
from jax.experimental import pallas as pl
from jax.experimental.pallas import tpu as pltpu
from jax.sharding import PartitionSpec as P

MESH = pl.DeviceIdType.MESH
EPSILON = 1e-05
BF16 = jnp.bfloat16
F32 = jnp.float32
GROUP = 2
UP, DOWN = 0, 1
Q1, Q2, K1, K2, V1 = range(5)


def when(condition):
    return pl.when(condition)


def branches(index, count, body):
    for k in range(count):
        pl.when(index == k)(functools.partial(body, k))


def xor(left, bits):
    result, weight = 0, 1
    while bits:
        low = lax.rem(lax.div(left, weight), 2)
        result = result + weight * (1 - low if bits % 2 else low)
        bits, weight = bits // 2, weight * 2
    return result + left - lax.rem(left, weight)


def aligned(value, unit):
    return pl.multiple_of(value, unit)


def layer_norm(rows, scales):
    average = jnp.mean(rows, axis=-1, keepdims=True)
    centred = rows - average
    spread = jnp.mean(centred * centred, axis=-1, keepdims=True)
    return centred * lax.rsqrt(spread + EPSILON) * scales


def combo_order(heads):
    order = []
    for h in range(heads):
        order += [(0, h), (1, h)] if h % 2 == 0 else [(1, h), (0, h)]
    return order


class Sizes:
    def __init__(self, n_sp, n_tp, heads, tokens, value, width, sub, hidden):
        self.n_sp, self.n_tp, self.heads = n_sp, n_tp, heads
        self.combos = combo_order(heads)
        self.A = len(self.combos)
        self.B = n_sp // self.A
        self.F = n_sp // GROUP
        self.tokens, self.value = tokens, value
        self.rows = tokens // n_tp
        self.width, self.sub = width, sub
        self.hidden = hidden // GROUP
        self.chips = GROUP * n_tp // 2
        self.order = range(self.A - 1, 0, -1)


def slots(kind):
    return (Q1, K1, V1) if kind == 0 else (Q1, Q2, K1, K2, V1)


def body(
    z,
    scales,
    query_block,
    key_block,
    lam_ref,
    gain_ref,
    norm_ref,
    residual_ref,
    qf,
    kf,
    vf,
    qs,
    ks,
    vs,
    ow_in,
    up_in,
    down_in,
    out_ref,
    qb,
    kb,
    vw,
    head_out,
    gathered,
    ow,
    wup,
    wdn,
    x_all,
    normed_ref,
    own_part,
    s1_out,
    s1_in,
    s2_out,
    s2_in,
    qkv_send,
    qkv_recv,
    kv_send,
    kv_recv,
    local_sem,
    swap_send,
    swap_recv,
    wz_send,
    wz_recv,
    wlocal_sem,
    ow_send,
    ow_recv,
    owlocal_sem,
    o_send,
    o_recv,
    x_send,
    xf_send,
    x_recv,
    s1_send,
    s1_recv,
    s2_send,
    s2_recv,
):
    s, t = lax.axis_index("sp"), lax.axis_index("tp")
    A, B, F, n_sp, n_tp = z.A, z.B, z.F, z.n_sp, z.n_tp
    a, b = lax.div(s, B), lax.rem(s, B)
    f, g = lax.div(s, GROUP), lax.rem(s, GROUP)
    chip, core = g * (n_tp // 2) + lax.div(t, 2), lax.rem(t, 2)
    pair = (s, t + 1 - 2 * core)
    TD, VD, R, sub, hidden = z.tokens, z.value, z.rows, z.sub, z.hidden
    half = qb.shape[2]

    def remote(src, dst, send, recv, device):
        return pltpu.make_async_remote_copy(
            src_ref=src, dst_ref=dst, send_sem=send, recv_sem=recv, device_id=device, device_id_type=MESH
        )

    vw[:, VD:] = jnp.ones((vw.shape[0], VD), BF16)
    barrier = pltpu.get_barrier_semaphore()
    for i in range(n_sp):
        for j in range(n_tp):
            @when((s != i) | (t != j))
            def greet():
                pl.semaphore_signal(barrier, inc=1, device_id=(i, j), device_id_type=MESH)
    pl.semaphore_wait(barrier, n_sp * n_tp - 1)

    def source(i, slot):
        kind, h = z.combos[i]
        if kind == 0:
            return {Q1: qf, K1: kf, V1: vf}[slot].at[h]
        if slot == V1:
            return vs.at[h]
        return (qs if slot < K1 else ks).at[h, slot % 2]

    def target(slot, origin, member):
        if slot < K1:
            return qb.at[slot, pl.ds(aligned(origin * TD, TD), TD), :]
        row = pl.ds(aligned((origin * B + member) * TD, TD), TD)
        if slot < V1:
            return kb.at[slot - K1, row, :]
        return vw.at[row, pl.ds(0, VD)]

    def qkv(me, i, slot):
        return remote(
            source(i, slot), target(slot, me, b), qkv_send.at[i, slot], qkv_recv.at[me, slot], (i * B + b, t)
        )

    def qkv_arrival(origin, slot):
        place = target(slot, origin, b)
        return remote(place, place, qkv_send.at[0, slot], qkv_recv.at[origin, slot], (s, t))

    def qkv_local(me, slot):
        return pltpu.make_async_copy(source(me, slot), target(slot, me, b), local_sem.at[slot])

    def kv(me, origin, other, slot):
        src = source(me, slot) if origin == me else target(slot, origin, b)
        return remote(
            src, target(slot, origin, b), kv_send.at[origin, other, slot - K1], kv_recv.at[origin, b, slot - K1],
            (me * B + other, t),
        )

    def kv_arrival(origin, member, slot):
        place = target(slot, origin, member)
        return remote(place, place, kv_send.at[0, 0, 0], kv_recv.at[origin, member, slot - K1], (s, t))

    def peers(count, mine, action):
        for k in range(count):
            pl.when(mine != k)(functools.partial(action, k))

    def near(me):
        return sorted((i for i in range(A) if i != me), key=lambda i: abs(i - me))

    @functools.partial(branches, a, A)
    def send_heads(me):
        for i in reversed(near(me)):
            for slot in reversed(slots(z.combos[i][0])):
                qkv(me, i, slot).start()
        mine = slots(z.combos[me][0])
        for slot in mine:
            qkv_local(me, slot).start()

        def share(other):
            for slot in mine:
                if slot >= K1:
                    kv(me, me, other, slot).start()

        peers(B, b, share)

    def wplace(kind, block):
        if kind == UP:
            return wup.at[pl.ds(aligned(block * sub, sub), sub), :]
        return wdn.at[block]

    def wsource(kind, half):
        window = pl.ds(aligned(half * hidden, hidden), hidden)
        return up_in.at[:, window] if kind == UP else down_in.at[window, :]

    def swap(kind):
        return remote(
            wsource(kind, 1 - g), wplace(kind, s), swap_send.at[kind], swap_recv.at[kind], (f * GROUP + 1 - g, t)
        )

    def swap_arrival(kind):
        place = wplace(kind, f * GROUP + 1 - g)
        return remote(place, place, swap_send.at[kind], swap_recv.at[kind], (s, t))

    def wlocal(kind):
        return pltpu.make_async_copy(wsource(kind, g), wplace(kind, s), wlocal_sem.at[kind])

    def along(me, origin, index, kind, direction, raw=False):
        j = g if index == 0 else 1 - g
        place = wplace(kind, origin * GROUP + j)
        src = wsource(kind, g) if raw else place
        return remote(
            src, place, wz_send.at[(direction + 1) // 2, origin, index, kind], wz_recv.at[origin, index, kind],
            ((me + direction) * GROUP + g, t),
        )

    def relay(events):
        if not events:
            return

        @functools.partial(branches, f, F)
        def pass_on(me):
            for k, index, kind in events:
                for direction in (1, -1):
                    origin = me - direction * k
                    if 0 <= origin < F:
                        move = along(me, origin, index, kind, direction)
                        move.wait_recv()
                        if 0 <= me + direction < F:
                            move.start()

    events = [(k, index, kind) for k in range(1, F) for index in range(2) for kind in (UP, DOWN)]

    for kind in (UP, DOWN):
        swap(kind).start()
        wlocal(kind).start()

    @functools.partial(branches, f, F)
    def send_own(me):
        for kind in (UP, DOWN):
            for direction in (1, -1):
                if 0 <= me + direction < F:
                    along(me, me, 0, kind, direction, raw=True).start()

    def ow_rows(i):
        kind, h = z.combos[i]
        return ow_in.at[pl.ds((kind * z.heads + h) * VD, VD), :]

    def ow_place(owner, i):
        return ow.at[pl.ds(aligned((owner * A + i) * VD, VD), VD), :]

    def ow_copy(i, other):
        return remote(ow_rows(i), ow_place(t, i), ow_send.at[other, i], ow_recv.at[t, i], (s, other))

    def ow_local(i):
        return pltpu.make_async_copy(ow_rows(i), ow_place(t, i), owlocal_sem.at[i])

    def ow_arrival(owner, i):
        place = ow_place(owner, i)
        return remote(place, place, ow_send.at[0, 0], ow_recv.at[owner, i], (s, t))

    for i in range(A):
        ow_local(i).start()
    peers(n_tp, t, lambda other: [ow_copy(i, other).start() for i in range(A)] and None)

    @functools.partial(branches, a, A)
    def receive_heads(me):
        mine = slots(z.combos[me][0])
        for origin in near(me):
            for slot in mine:
                if slot >= K1:
                    qkv_arrival(origin, slot).wait_recv()

            def share(other):
                for slot in mine:
                    if slot >= K1:
                        kv(me, origin, other, slot).start()

            peers(B, b, share)

    for kind in (UP, DOWN):
        swap_arrival(kind).wait_recv()

    @functools.partial(branches, f, F)
    def send_swapped(me):
        for kind in (UP, DOWN):
            for direction in (1, -1):
                if 0 <= me + direction < F:
                    along(me, me, 1, kind, direction).start()

    @functools.partial(branches, a, A)
    def receive_rest(me):
        mine = slots(z.combos[me][0])
        for slot in mine:
            qkv_local(me, slot).wait()
            if slot < K1:
                for origin in near(me):
                    qkv_arrival(origin, slot).wait_recv()
            else:
                for origin in range(A):
                    peers(B, b, lambda other: kv_arrival(origin, other, slot).wait_recv())

    second = sum(jnp.where(a == i, kind, 0) for i, (kind, h) in enumerate(z.combos))

    @when(second == 0)
    def split_maps():
        low = lax.broadcasted_iota(jnp.int32, (TD, half), 1) < half // 2
        for block in range(A):
            rows = pl.ds(block * TD, TD)
            queries = qb[0, rows, :]
            empty = jnp.zeros_like(queries)
            qb[1, rows, :] = jnp.where(low, empty, queries)
            qb[0, rows, :] = jnp.where(low, queries, empty)

    factor = jnp.where(second == 0, scales[0], scales[1]) * math.log2(math.e)
    lam = lam_ref[a]
    gain = gain_ref[pl.ds(a, 1), :]

    def attend(row):
        maxima, sums = [None, None], [None, None]
        window = pl.ds(aligned(row, query_block), query_block)
        for start in range(0, n_sp * TD, key_block):
            for c in range(2):
                scores = lax.dot_general(
                    qb[c, window, :],
                    kb[second * c, start : start + key_block, :],
                    (((1,), (1,)), ((), ())),
                    preferred_element_type=F32,
                )
                newest = jnp.max(scores, axis=-1, keepdims=True)
                if start:
                    newest = jnp.maximum(maxima[c], newest)
                weights = jnp.exp2((scores - newest) * factor).astype(BF16)
                summed = jnp.dot(weights, vw[start : start + key_block, :], preferred_element_type=F32)
                if start:
                    summed = summed + sums[c] * jnp.exp2((maxima[c] - newest) * factor)
                maxima[c], sums[c] = newest, summed
        one, two = (member[:, :VD] / member[:, VD:] for member in sums)
        attended = one - lam * two
        mean_square = jnp.mean(attended * attended, axis=-1, keepdims=True)
        head_out[window, :] = (attended * lax.rsqrt(mean_square + EPSILON) * gain).astype(BF16)

    def outs(n, owner, other):
        rows = pl.ds(aligned(owner * TD + other * R, R), R)
        return remote(
            head_out.at[rows, :], gathered.at[t * A + a], o_send.at[n, other], o_recv.at[t * A + a],
            (owner * B + b, other),
        )

    def outs_arrival(index):
        place = gathered.at[index]
        return remote(place, place, o_send.at[0, 0], o_recv.at[index], (s, t))

    early = {0: events[0:2], 1: events[2:3], 2: events[3:4], 3: events[4:6]}

    def attention_step(n, carry):
        owner = lax.rem(a + 1 + n, A)

        def inner(m, unused):
            attend(owner * TD + m * query_block)
            return unused

        lax.fori_loop(0, TD // query_block, inner, 0)
        for other in range(n_tp):
            @when((n < A - 1) | (t != other))
            def send():
                outs(n, owner, other).start()
        for point in range(min(A, len(early))):
            pl.when(n == point)(functools.partial(relay, early[point]))
        return carry

    lax.fori_loop(0, A, attention_step, 0)
    gathered[t * A + a] = head_out[pl.ds(aligned(a * TD + t * R, R), R), :]
    used = sum(len(early[point]) for point in range(min(A, len(early))))

    for i in range(A):
        ow_local(i).wait()
    for owner in range(n_tp):
        @when(t != owner)
        def weights_arrive():
            for i in range(A):
                ow_arrival(owner, i).wait_recv()
    for index in range(n_tp * A):
        pl.when((t != index // A) | (a != index % A))(lambda: outs_arrival(index).wait_recv())

    left = jnp.concatenate([gathered[index] for index in range(n_tp * A)], axis=1)
    projected = jnp.dot(left, ow[...], preferred_element_type=F32) + residual_ref[...].astype(F32)
    normed = layer_norm(projected, norm_ref[0:1, :])
    normed_ref[...] = normed
    x_all[chip * 2 + core] = normed.astype(BF16)

    def chip_at(n):
        return xor(chip, n)

    def device_of(index, c):
        return (f * GROUP + lax.div(index, n_tp // 2), lax.rem(index, n_tp // 2) * 2 + c)

    def rows_to_chip(n):
        place = x_all.at[chip * 2 + core]
        return remote(place, place, x_send.at[n], x_recv.at[chip * 2 + core], device_of(chip_at(n), core))

    def rows_to_pair(n):
        index = chip_at(n) * 2 + core
        return remote(x_all.at[index], x_all.at[index], xf_send.at[n], x_recv.at[index], pair)

    def rows_arrival(index):
        place = x_all.at[index]
        return remote(place, place, x_send.at[0], x_recv.at[index], (s, t))

    rows_to_pair(0).start()
    for n in range(z.chips - 1, 0, -1):
        rows_to_chip(n).start()

    relay(events[used:])
    for kind in (UP, DOWN):
        wlocal(kind).wait()

    def half_to_pair(n):
        return remote(s1_out.at[n], s1_in.at[n], s1_send.at[n], s1_recv.at[n], pair)

    def sum_to_chip(n):
        return remote(s2_out.at[n], s2_in.at[n], s2_send.at[n], s2_recv.at[n], device_of(chip_at(n), core))

    def feed(n):
        index = chip_at(n)
        if n:
            rows_arrival(index * 2 + core).wait_recv()
            rows_to_pair(n).start()
        rows_arrival(index * 2 + 1 - core).wait_recv()
        for c in range(2):
            expanded = jnp.dot(x_all[index * 2 + c], wup[...], preferred_element_type=F32)
            acted = jnp.square(jnp.maximum(expanded, 0.0)).astype(BF16)

            def columns(block, unused):
                part = jnp.dot(acted, wdn[block], preferred_element_type=F32)
                window = pl.ds(aligned(block * sub, sub), sub)

                @when(core == c)
                def keep():
                    own_part[n, :, window] = part

                @when(core != c)
                def give():
                    s1_out[n, :, window] = part.astype(BF16)

                return unused

            for block in range(n_sp):
                columns(block, 0)
        half_to_pair(n).start()

    def reduce(n):
        half_to_pair(n).wait_recv()
        s2_out[n] = (own_part[n] + s1_in[n].astype(F32)).astype(BF16)
        sum_to_chip(n).start()

    for n in range(z.chips):
        feed(n)
        if n > 1:
            reduce(n - 1)
    reduce(z.chips - 1)

    half_to_pair(0).wait_recv()
    total = normed_ref[...] + own_part[0] + s1_in[0].astype(F32)
    for n in range(1, z.chips):
        sum_to_chip(n).wait_recv()
        total = total + s2_in[n].astype(F32)
    out_ref[...] = layer_norm(total, norm_ref[1:2, :]).astype(BF16)

    @functools.partial(branches, a, A)
    def drain_heads(me):
        for i in near(me):
            for slot in slots(z.combos[i][0]):
                qkv(me, i, slot).wait_send()

        def drain(other):
            for slot in slots(z.combos[me][0]):
                if slot >= K1:
                    for origin in range(A):
                        kv(me, origin, other, slot).wait_send()

        peers(B, b, drain)

    for kind in (UP, DOWN):
        swap(kind).wait_send()

    @functools.partial(branches, f, F)
    def drain_weights(me):
        for direction in (1, -1):
            if 0 <= me + direction < F:
                for k in range(F):
                    origin = me - direction * k
                    if 0 <= origin < F:
                        for index in range(2):
                            for kind in (UP, DOWN):
                                along(me, origin, index, kind, direction).wait_send()

    peers(n_tp, t, lambda other: [ow_copy(i, other).wait_send() for i in range(A)] and None)
    for n in range(A):
        for other in range(n_tp):
            if n < A - 1:
                outs(n, lax.rem(a + 1 + n, A), other).wait_send()
            else:
                pl.when(t != other)(lambda: outs(n, a, other).wait_send())
    for n in range(z.chips):
        rows_to_pair(n).wait_send()
        half_to_pair(n).wait_send()
        if n:
            rows_to_chip(n).wait_send()
            sum_to_chip(n).wait_send()


def local(
    query_first,
    key_first,
    value_first,
    query_second,
    key_second,
    value_second,
    mix_lambda,
    head_gain,
    out_weight,
    residual,
    norm_gain,
    up_weight,
    down_weight,
    n_sp,
    n_tp,
):
    tokens, heads, width_first = query_first.shape
    width_second = query_second.shape[2]
    value = value_first.shape[2]
    width, hidden = up_weight.shape[0] * n_sp, up_weight.shape[1]
    sub = up_weight.shape[0]
    z = Sizes(n_sp, n_tp, heads, tokens, value, width, sub, hidden)
    half = width_second // 2

    def by_head(array):
        return array.transpose(1, 0, 2)

    def by_map(array):
        return array.reshape(tokens, heads, 2, half).transpose(1, 2, 0, 3)

    lam = jnp.stack([mix_lambda[kind, h] for kind, h in z.combos])
    gains = jnp.stack([head_gain[kind, h] for kind, h in z.combos])
    query_block = next(k for k in (384, 256, 128, tokens) if tokens % k == 0)
    key_block = next(k for k in (1024, 512, 256, tokens) if (n_sp * tokens) % k == 0)
    kernel = functools.partial(
        body, z, (1.0 / math.sqrt(width_first // 2), 1.0 / math.sqrt(half)), query_block, key_block
    )
    total = n_sp * tokens
    rows, A, B, F, chips = z.rows, z.A, z.B, z.F, z.chips
    DMA = pltpu.SemaphoreType.DMA
    vmem = pl.BlockSpec(memory_space=pltpu.VMEM)
    anywhere = pl.BlockSpec(memory_space=pl.ANY)
    return pl.pallas_call(
        kernel,
        in_specs=[pl.BlockSpec(memory_space=pltpu.SMEM), vmem, vmem, vmem] + [anywhere] * 9,
        out_specs=vmem,
        out_shape=jax.ShapeDtypeStruct((rows, width), BF16),
        scratch_shapes=[
            pltpu.VMEM((2, A * tokens, half), BF16),
            pltpu.VMEM((2, total, half), BF16),
            pltpu.VMEM((total, 2 * value), BF16),
            pltpu.VMEM((A * tokens, value), BF16),
            pltpu.VMEM((n_tp * A, rows, value), BF16),
            pltpu.VMEM((n_tp * A * value, width), BF16),
            pltpu.VMEM((width, z.hidden), BF16),
            pltpu.VMEM((n_sp, z.hidden, sub), BF16),
            pltpu.VMEM((2 * chips, rows, width), BF16),
            pltpu.VMEM((rows, width), F32),
            pltpu.VMEM((chips, rows, width), F32),
            pltpu.VMEM((chips, rows, width), BF16),
            pltpu.VMEM((chips, rows, width), BF16),
            pltpu.VMEM((chips, rows, width), BF16),
            pltpu.VMEM((chips, rows, width), BF16),
            DMA((A, 5)),
            DMA((A, 5)),
            DMA((A, B, 3)),
            DMA((A, B, 3)),
            DMA((5,)),
            DMA((2,)),
            DMA((2,)),
            DMA((2, F, 2, 2)),
            DMA((F, 2, 2)),
            DMA((2,)),
            DMA((n_tp, A)),
            DMA((n_tp, A)),
            DMA((A,)),
            DMA((A, n_tp)),
            DMA((n_tp * A,)),
            DMA((chips,)),
            DMA((chips,)),
            DMA((2 * chips,)),
            DMA((chips,)),
            DMA((chips,)),
            DMA((chips,)),
            DMA((chips,)),
        ],
        compiler_params=pltpu.CompilerParams(
            collective_id=0, has_side_effects=True, vmem_limit_bytes=67043328
        ),
    )(
        lam,
        gains,
        norm_gain,
        residual,
        by_head(query_first),
        by_head(key_first),
        by_head(value_first),
        by_map(query_second),
        by_map(key_second),
        by_head(value_second),
        out_weight.reshape(-1, width),
        up_weight,
        down_weight,
    )


def solution(mesh):
    return jax.shard_map(
        functools.partial(local, n_sp=mesh.shape["sp"], n_tp=mesh.shape["tp"]),
        mesh=mesh,
        in_specs=(
            P("sp", "tp", None),
            P("sp", "tp", None),
            P("sp", "tp", None),
            P("sp", "tp", None),
            P("sp", "tp", None),
            P("sp", "tp", None),
            P(None, "tp"),
            P(None, "tp", None),
            P(None, "tp", None, None),
            P(("sp", "tp"), None),
            P(),
            P("sp", "tp"),
            P("tp", "sp"),
        ),
        out_specs=P(("sp", "tp"), None),
        check_vma=False,
    )
```

```python
import functools
import math

import jax
import jax.numpy as jnp
from jax import lax
from jax.experimental import pallas as pl
from jax.experimental.pallas import tpu as pltpu
from jax.sharding import PartitionSpec as P

MESH = pl.DeviceIdType.MESH
EPSILON = 1e-05
BF16 = jnp.bfloat16
F32 = jnp.float32
GROUP = 2
UP, DOWN = 0, 1
Q1, Q2, K1, K2, V1 = range(5)


def when(condition):
    return pl.when(condition)


def branches(index, count, body):
    for k in range(count):
        pl.when(index == k)(functools.partial(body, k))


def xor(left, bits):
    result, weight = 0, 1
    while bits:
        low = lax.rem(lax.div(left, weight), 2)
        result = result + weight * (1 - low if bits % 2 else low)
        bits, weight = bits // 2, weight * 2
    return result + left - lax.rem(left, weight)


def aligned(value, unit):
    return pl.multiple_of(value, unit)


def layer_norm(rows, scales):
    average = jnp.mean(rows, axis=-1, keepdims=True)
    centred = rows - average
    spread = jnp.mean(centred * centred, axis=-1, keepdims=True)
    return centred * lax.rsqrt(spread + EPSILON) * scales


def combo_order(heads):
    order = []
    for h in range(heads):
        order += [(0, h), (1, h)] if h % 2 == 0 else [(1, h), (0, h)]
    return order


class Sizes:
    def __init__(self, n_sp, n_tp, heads, tokens, value, width, sub, hidden):
        self.n_sp, self.n_tp, self.heads = n_sp, n_tp, heads
        self.combos = combo_order(heads)
        self.A = len(self.combos)
        self.B = n_sp // self.A
        self.F = n_sp // GROUP
        self.tokens, self.value = tokens, value
        self.rows = tokens // n_tp
        self.width, self.sub = width, sub
        self.hidden = hidden // GROUP
        self.chips = GROUP * n_tp // 2
        self.order = range(self.A - 1, 0, -1)


def slots(kind):
    return (Q1, K1, V1) if kind == 0 else (Q1, Q2, K1, K2, V1)


def body(
    z,
    scales,
    query_block,
    key_block,
    lam_ref,
    gain_ref,
    norm_ref,
    residual_in,
    qf,
    kf,
    vf,
    qs,
    ks,
    vs,
    ow_in,
    up_in,
    down_in,
    out_ref,
    qb,
    kb,
    vw,
    head_out,
    gathered,
    ow,
    wup,
    wdn,
    x_all,
    normed_ref,
    residual_ref,
    own_part,
    s1_out,
    s1_in,
    s2_out,
    s2_in,
    qkv_send,
    qkv_recv,
    kv_send,
    kv_recv,
    local_sem,
    swap_send,
    swap_recv,
    wz_send,
    wz_recv,
    wlocal_sem,
    ow_send,
    ow_recv,
    owlocal_sem,
    o_send,
    o_recv,
    x_send,
    xf_send,
    x_recv,
    xh_send,
    xh_recv,
    residual_sem,
    s1_send,
    s1_recv,
    s2_send,
    s2_recv,
):
    s, t = lax.axis_index("sp"), lax.axis_index("tp")
    A, B, F, n_sp, n_tp = z.A, z.B, z.F, z.n_sp, z.n_tp
    a, b = lax.div(s, B), lax.rem(s, B)
    f, g = lax.div(s, GROUP), lax.rem(s, GROUP)
    chip, core = g * (n_tp // 2) + lax.div(t, 2), lax.rem(t, 2)
    pair = (s, t + 1 - 2 * core)
    TD, VD, R, sub, hidden = z.tokens, z.value, z.rows, z.sub, z.hidden
    half = qb.shape[2]

    def remote(src, dst, send, recv, device):
        return pltpu.make_async_remote_copy(
            src_ref=src, dst_ref=dst, send_sem=send, recv_sem=recv, device_id=device, device_id_type=MESH
        )

    vw[:, VD:] = jnp.ones((vw.shape[0], VD), BF16)
    barrier = pltpu.get_barrier_semaphore()
    for i in range(n_sp):
        for j in range(n_tp):
            @when((s != i) | (t != j))
            def greet():
                pl.semaphore_signal(barrier, inc=1, device_id=(i, j), device_id_type=MESH)
    pl.semaphore_wait(barrier, n_sp * n_tp - 1)

    def source(i, slot):
        kind, h = z.combos[i]
        if kind == 0:
            return {Q1: qf, K1: kf, V1: vf}[slot].at[h]
        if slot == V1:
            return vs.at[h]
        return (qs if slot < K1 else ks).at[h, slot % 2]

    def target(slot, origin, member):
        if slot < K1:
            return qb.at[slot, pl.ds(aligned(origin * TD, TD), TD), :]
        row = pl.ds(aligned((origin * B + member) * TD, TD), TD)
        if slot < V1:
            return kb.at[slot - K1, row, :]
        return vw.at[row, pl.ds(0, VD)]

    def qkv(me, i, slot):
        return remote(
            source(i, slot), target(slot, me, b), qkv_send.at[i, slot], qkv_recv.at[me, slot], (i * B + b, t)
        )

    def qkv_arrival(origin, slot):
        place = target(slot, origin, b)
        return remote(place, place, qkv_send.at[0, slot], qkv_recv.at[origin, slot], (s, t))

    def qkv_local(me, slot):
        return pltpu.make_async_copy(source(me, slot), target(slot, me, b), local_sem.at[slot])

    def kv(me, origin, other, slot):
        src = source(me, slot) if origin == me else target(slot, origin, b)
        return remote(
            src, target(slot, origin, b), kv_send.at[origin, other, slot - K1], kv_recv.at[origin, b, slot - K1],
            (me * B + other, t),
        )

    def kv_arrival(origin, member, slot):
        place = target(slot, origin, member)
        return remote(place, place, kv_send.at[0, 0, 0], kv_recv.at[origin, member, slot - K1], (s, t))

    def peers(count, mine, action):
        for k in range(count):
            pl.when(mine != k)(functools.partial(action, k))

    def near(me):
        return sorted((i for i in range(A) if i != me), key=lambda i: abs(i - me))

    @functools.partial(branches, a, A)
    def send_heads(me):
        for i in near(me):
            for slot in slots(z.combos[i][0]):
                if slot >= K1:
                    qkv(me, i, slot).start()
        for n in range(1, A):
            i = (me - n) % A
            for slot in slots(z.combos[i][0]):
                if slot < K1:
                    qkv(me, i, slot).start()
        mine = slots(z.combos[me][0])

        def share(other):
            for slot in mine:
                if slot >= K1:
                    kv(me, me, other, slot).start()

        peers(B, b, share)
        for slot in mine:
            qkv_local(me, slot).start()

    def wplace(kind, block):
        if kind == UP:
            return wup.at[pl.ds(aligned(block * sub, sub), sub), :]
        return wdn.at[block]

    def wsource(kind, half):
        window = pl.ds(aligned(half * hidden, hidden), hidden)
        return up_in.at[:, window] if kind == UP else down_in.at[window, :]

    def swap(kind):
        return remote(
            wsource(kind, 1 - g), wplace(kind, s), swap_send.at[kind], swap_recv.at[kind], (f * GROUP + 1 - g, t)
        )

    def swap_arrival(kind):
        place = wplace(kind, f * GROUP + 1 - g)
        return remote(place, place, swap_send.at[kind], swap_recv.at[kind], (s, t))

    def wlocal(kind):
        return pltpu.make_async_copy(wsource(kind, g), wplace(kind, s), wlocal_sem.at[kind])

    def along(me, origin, index, kind, direction, raw=False):
        j = g if index == 0 else 1 - g
        place = wplace(kind, origin * GROUP + j)
        src = wsource(kind, g) if raw else place
        return remote(
            src, place, wz_send.at[(direction + 1) // 2, origin, index, kind], wz_recv.at[origin, index, kind],
            ((me + direction) * GROUP + g, t),
        )

    def relay(events):
        if not events:
            return

        @functools.partial(branches, f, F)
        def pass_on(me):
            for k, index, kind in events:
                if k == 0:
                    swap_arrival(kind).wait_recv()
                for direction in (1, -1):
                    origin = me - direction * k
                    if 0 <= origin < F:
                        if k:
                            along(me, origin, index, kind, direction).wait_recv()
                        if 0 <= me + direction < F:
                            along(me, origin, index, kind, direction).start()

    first = [(0, 1, UP), (0, 1, DOWN), (1, 0, UP), (1, 1, UP), (1, 0, DOWN)]
    rest = [(k, index, UP) for k in range(1, F - 1) for index in range(2)]
    rest += [(k, index, DOWN) for k in range(1, F - 1) for index in range(2)]
    events = first + [event for event in rest if event not in first]
    last = [[(F - 1, index, kind) for index in range(2)] for kind in (UP, DOWN)]

    for kind in (UP, DOWN):
        wlocal(kind).start()
    pltpu.make_async_copy(residual_in, residual_ref, residual_sem.at[0]).start()

    @functools.partial(branches, f, F)
    def send_own(me):
        for kind in (UP, DOWN):
            for direction in (1, -1):
                if 0 <= me + direction < F:
                    along(me, me, 0, kind, direction, raw=True).start()

    def ow_rows(i):
        kind, h = z.combos[i]
        return ow_in.at[pl.ds((kind * z.heads + h) * VD, VD), :]

    def ow_place(owner, i):
        return ow.at[pl.ds(aligned((owner * A + i) * VD, VD), VD), :]

    def ow_copy(i, other):
        return remote(ow_rows(i), ow_place(t, i), ow_send.at[other, i], ow_recv.at[t, i], (s, other))

    def ow_local(i):
        return pltpu.make_async_copy(ow_rows(i), ow_place(t, i), owlocal_sem.at[i])

    def ow_arrival(owner, i):
        place = ow_place(owner, i)
        return remote(place, place, ow_send.at[0, 0], ow_recv.at[owner, i], (s, t))

    for i in range(A):
        ow_local(i).start()
    peers(n_tp, t, lambda other: [ow_copy(i, other).start() for i in range(A)] and None)

    @functools.partial(branches, a, A)
    def receive_heads(me):
        mine = slots(z.combos[me][0])
        for origin in near(me):
            for slot in mine:
                if slot >= K1:
                    qkv_arrival(origin, slot).wait_recv()

            def share(other):
                for slot in mine:
                    if slot >= K1:
                        kv(me, origin, other, slot).start()

            peers(B, b, share)

    for kind in (UP, DOWN):
        swap(kind).start()

    @functools.partial(branches, a, A)
    def receive_rest(me):
        mine = slots(z.combos[me][0])
        for slot in mine:
            qkv_local(me, slot).wait()
            if slot >= K1:
                for origin in range(A):
                    peers(B, b, lambda other: kv_arrival(origin, other, slot).wait_recv())

    second = sum(jnp.where(a == i, kind, 0) for i, (kind, h) in enumerate(z.combos))

    def queries_of(origin):
        @when(origin != a)
        def arrive():
            qkv_arrival(origin, Q1).wait_recv()
            pl.when(second == 1)(lambda: qkv_arrival(origin, Q2).wait_recv())

        @when(second == 0)
        def split_maps():
            low = lax.broadcasted_iota(jnp.int32, (TD, half), 1) < half // 2
            rows = pl.ds(aligned(origin * TD, TD), TD)
            queries = qb[0, rows, :]
            empty = jnp.zeros_like(queries)
            qb[1, rows, :] = jnp.where(low, empty, queries)
            qb[0, rows, :] = jnp.where(low, queries, empty)

    factor = jnp.where(second == 0, scales[0], scales[1]) * math.log2(math.e)
    lam = sum(jnp.where(a == i, lam_ref[kind, h], 0.0) for i, (kind, h) in enumerate(z.combos))
    gain = sum(jnp.where(a == i, gain_ref[kind, h : h + 1, :], 0.0) for i, (kind, h) in enumerate(z.combos))

    def attend(row):
        maxima, sums = [None, None], [None, None]
        window = pl.ds(aligned(row, query_block), query_block)
        for start in range(0, n_sp * TD, key_block):
            for c in range(2):
                scores = lax.dot_general(
                    qb[c, window, :],
                    kb[second * c, start : start + key_block, :],
                    (((1,), (1,)), ((), ())),
                    preferred_element_type=F32,
                )
                newest = jnp.max(scores, axis=-1, keepdims=True)
                if start:
                    newest = jnp.maximum(maxima[c], newest)
                weights = jnp.exp2((scores - newest) * factor).astype(BF16)
                summed = jnp.dot(weights, vw[start : start + key_block, :], preferred_element_type=F32)
                if start:
                    summed = summed + sums[c] * jnp.exp2((maxima[c] - newest) * factor)
                maxima[c], sums[c] = newest, summed
        one, two = (member[:, :VD] / member[:, VD:] for member in sums)
        attended = one - lam * two
        mean_square = jnp.mean(attended * attended, axis=-1, keepdims=True)
        head_out[window, :] = (attended * lax.rsqrt(mean_square + EPSILON) * gain).astype(BF16)

    def outs(n, owner, other):
        rows = pl.ds(aligned(owner * TD + other * R, R), R)
        return remote(
            head_out.at[rows, :], gathered.at[t * A + a], o_send.at[n, other], o_recv.at[t * A + a],
            (owner * B + b, other),
        )

    def outs_arrival(index):
        place = gathered.at[index]
        return remote(place, place, o_send.at[0, 0], o_recv.at[index], (s, t))

    blocks = TD // query_block
    plan = {0: events[0:1], 2: events[1:2], 4: events[2:3], 5: events[3:4], 7: events[4:5]}
    plan = {point: moves for point, moves in plan.items() if point < A * blocks}
    pending = [event for event in events if not any(event in moves for moves in plan.values())]

    def attention_step(n, carry):
        owner = lax.rem(a + n, A)
        queries_of(owner)

        def inner(m, unused):
            attend(owner * TD + m * query_block)
            for point, moves in plan.items():
                pl.when(n * blocks + m == point)(functools.partial(relay, moves))
            return unused

        lax.fori_loop(0, blocks, inner, 0)
        for other in range(n_tp):
            @when((n > 0) | (t != other))
            def send():
                outs(n, owner, other).start()
        return carry

    lax.fori_loop(0, A, attention_step, 0)
    gathered[t * A + a] = head_out[pl.ds(aligned(a * TD + t * R, R), R), :]
    relay(pending[:1])
    pltpu.make_async_copy(residual_in, residual_ref, residual_sem.at[0]).wait()

    for i in range(A):
        ow_local(i).wait()
    for owner in range(n_tp):
        @when(t != owner)
        def weights_arrive():
            for i in range(A):
                ow_arrival(owner, i).wait_recv()
    for index in range(n_tp * A):
        pl.when((t != index // A) | (a != index % A))(lambda: outs_arrival(index).wait_recv())

    left = jnp.concatenate([gathered[index] for index in range(n_tp * A)], axis=1)
    projected = jnp.dot(left, ow[...], preferred_element_type=F32) + residual_ref[...].astype(F32)
    normed = layer_norm(projected, norm_ref[0:1, :])
    normed_ref[...] = normed
    x_all[chip * 2 + core] = normed.astype(BF16)

    def chip_at(n):
        return xor(chip, n)

    def device_of(index, c):
        return (f * GROUP + lax.div(index, n_tp // 2), lax.rem(index, n_tp // 2) * 2 + c)

    def rows_to_chip(n):
        place = x_all.at[chip * 2 + core]
        return remote(place, place, x_send.at[n], x_recv.at[chip * 2 + core], device_of(chip_at(n), core))

    def rows_to_pair(n):
        index = chip_at(n) * 2 + core
        return remote(x_all.at[index], x_all.at[index], xf_send.at[n], x_recv.at[index], pair)

    def rows_arrival(index):
        place = x_all.at[index]
        return remote(place, place, x_send.at[0], x_recv.at[index], (s, t))

    def half_rows(n, part, index):
        place = x_all.at[index, pl.ds(part * (R // 2), R // 2), :]
        return remote(place, place, xh_send.at[part], xh_recv.at[part], device_of(chip_at(n), core))

    square = z.chips == 4
    rows_to_pair(0).start()
    for n in range(1, 3 if square else z.chips):
        rows_to_chip(n).start()
    relay(pending[1:2])

    def rows_from_chip(n):
        index = chip_at(n) * 2 + core
        if square and n == 3:
            for part in range(2):
                half_rows(3, part, index).wait_recv()
        else:
            rows_arrival(index).wait_recv()
        if square and n < 3:
            half_rows(3 - n, n - 1, index).start()
        rows_to_pair(n).start()

    for n in range(1, 3 if square else z.chips):
        rows_from_chip(n)
    split = max([4] + [1 + i for i, event in enumerate(pending) if event[2] == UP])
    relay(pending[2:split])
    relay(last[UP])
    for kind in (UP, DOWN):
        wlocal(kind).wait()

    def expand(n):
        index = chip_at(n)
        rows_arrival(index * 2 + 1 - core).wait_recv()
        rows = x_all[pl.ds(index * 2, 2)].reshape(2 * R, x_all.shape[2])
        expanded = jnp.dot(rows, wup[...], preferred_element_type=F32)
        ow[n * 2 * R : (n + 1) * 2 * R, :hidden] = jnp.square(jnp.maximum(expanded, 0.0)).astype(BF16)

    for n in range(z.chips):
        if square and n == 3:
            rows_from_chip(3)
        expand(n)
    relay(pending[split:])

    orders = [sorted(range(F), key=lambda i: abs(i - me)) for me in range(F)]
    origins = [sum(jnp.where(f == me, orders[me][m], 0) for me in range(F)) for m in range(F)]
    parts = (range(F - 1), range(F - 1, F))

    def window(part):
        return pl.ds(parts[part][0], len(parts[part]))

    def half_to_pair(n, part):
        return remote(
            s1_out.at[n, window(part)], s1_in.at[n, window(part)], s1_send.at[n, part], s1_recv.at[n, part], pair
        )

    def sum_to_chip(n, part):
        return remote(
            s2_out.at[n, window(part)], s2_in.at[n, window(part)], s2_send.at[n, part], s2_recv.at[n, part],
            device_of(chip_at(n), core),
        )

    def contract(n, part):
        for m in parts[part]:
            for j in range(GROUP):
                columns = slice(j * sub, (j + 1) * sub)
                result = jnp.dot(
                    ow[n * 2 * R : (n + 1) * 2 * R, :hidden], wdn[origins[m] * GROUP + j], preferred_element_type=F32
                )
                for c in range(2):
                    piece = result[c * R : (c + 1) * R]

                    @when(core == c)
                    def keep():
                        own_part[n, m, :, columns] = piece

                    @when(core != c)
                    def give():
                        s1_out[n, m, :, columns] = piece.astype(BF16)

        half_to_pair(n, part).start()

    def reduce(n, part):
        half_to_pair(n, part).wait_recv()
        for m in parts[part]:
            s2_out[n, m] = (own_part[n, m] + s1_in[n, m].astype(F32)).astype(BF16)
        sum_to_chip(n, part).start()

    for part in range(2):
        if part:
            relay(last[DOWN])
        for n in range(z.chips - 1, -1, -1):
            contract(n, part)
            if n < z.chips - 1:
                reduce(n + 1, part)

    for part in range(2):
        half_to_pair(0, part).wait_recv()
        for n in range(1, z.chips):
            sum_to_chip(n, part).wait_recv()
        for m in parts[part]:
            columns = pl.ds(aligned(origins[m] * GROUP * sub, GROUP * sub), GROUP * sub)
            total = normed_ref[:, columns] + own_part[0, m] + s1_in[0, m].astype(F32)
            for n in range(1, z.chips):
                total = total + s2_in[n, m].astype(F32)
            normed_ref[:, columns] = total
    out_ref[...] = layer_norm(normed_ref[...], norm_ref[1:2, :]).astype(BF16)

    @functools.partial(branches, a, A)
    def drain_heads(me):
        for i in near(me):
            for slot in slots(z.combos[i][0]):
                qkv(me, i, slot).wait_send()

        def drain(other):
            for slot in slots(z.combos[me][0]):
                if slot >= K1:
                    for origin in range(A):
                        kv(me, origin, other, slot).wait_send()

        peers(B, b, drain)

    for kind in (UP, DOWN):
        swap(kind).wait_send()

    @functools.partial(branches, f, F)
    def drain_weights(me):
        for direction in (1, -1):
            if 0 <= me + direction < F:
                for k in range(F):
                    origin = me - direction * k
                    if 0 <= origin < F:
                        for index in range(2):
                            for kind in (UP, DOWN):
                                along(me, origin, index, kind, direction).wait_send()

    peers(n_tp, t, lambda other: [ow_copy(i, other).wait_send() for i in range(A)] and None)
    for n in range(A):
        for other in range(n_tp):
            if n:
                outs(n, lax.rem(a + n, A), other).wait_send()
            else:
                pl.when(t != other)(lambda: outs(n, a, other).wait_send())
    for n in range(z.chips):
        rows_to_pair(n).wait_send()
        for part in range(2):
            half_to_pair(n, part).wait_send()
            if n:
                sum_to_chip(n, part).wait_send()
        if n and not (square and n == 3):
            rows_to_chip(n).wait_send()
    if square:
        for n in (1, 2):
            half_rows(3 - n, n - 1, chip_at(n) * 2 + core).wait_send()


def local(
    query_first,
    key_first,
    value_first,
    query_second,
    key_second,
    value_second,
    mix_lambda,
    head_gain,
    out_weight,
    residual,
    norm_gain,
    up_weight,
    down_weight,
    n_sp,
    n_tp,
):
    tokens, heads, width_first = query_first.shape
    width_second = query_second.shape[2]
    value = value_first.shape[2]
    width, hidden = up_weight.shape[0] * n_sp, up_weight.shape[1]
    sub = up_weight.shape[0]
    z = Sizes(n_sp, n_tp, heads, tokens, value, width, sub, hidden)
    half = width_second // 2

    def by_head(array):
        return array.transpose(1, 0, 2)

    def by_map(array):
        return array.reshape(tokens, heads, 2, half).transpose(1, 2, 0, 3)

    query_block = next(k for k in (384, 256, 128, tokens) if tokens % k == 0)
    key_block = next(k for k in (1024, 512, 256, tokens) if (n_sp * tokens) % k == 0)
    kernel = functools.partial(
        body, z, (1.0 / math.sqrt(width_first // 2), 1.0 / math.sqrt(half)), query_block, key_block
    )
    total = n_sp * tokens
    rows, A, B, F, chips = z.rows, z.A, z.B, z.F, z.chips
    DMA = pltpu.SemaphoreType.DMA
    vmem = pl.BlockSpec(memory_space=pltpu.VMEM)
    anywhere = pl.BlockSpec(memory_space=pl.ANY)
    return pl.pallas_call(
        kernel,
        in_specs=[pl.BlockSpec(memory_space=pltpu.SMEM), vmem, vmem] + [anywhere] * 10,
        out_specs=vmem,
        out_shape=jax.ShapeDtypeStruct((rows, width), BF16),
        scratch_shapes=[
            pltpu.VMEM((2, A * tokens, half), BF16),
            pltpu.VMEM((2, total, half), BF16),
            pltpu.VMEM((total, 2 * value), BF16),
            pltpu.VMEM((A * tokens, value), BF16),
            pltpu.VMEM((n_tp * A, rows, value), BF16),
            pltpu.VMEM((n_tp * A * value, width), BF16),
            pltpu.VMEM((width, z.hidden), BF16),
            pltpu.VMEM((n_sp, z.hidden, sub), BF16),
            pltpu.VMEM((2 * chips, rows, width), BF16),
            pltpu.VMEM((rows, width), F32),
            pltpu.VMEM((rows, width), BF16),
            pltpu.VMEM((chips, F, rows, GROUP * sub), F32),
            pltpu.VMEM((chips, F, rows, GROUP * sub), BF16),
            pltpu.VMEM((chips, F, rows, GROUP * sub), BF16),
            pltpu.VMEM((chips, F, rows, GROUP * sub), BF16),
            pltpu.VMEM((chips, F, rows, GROUP * sub), BF16),
            DMA((A, 5)),
            DMA((A, 5)),
            DMA((A, B, 3)),
            DMA((A, B, 3)),
            DMA((5,)),
            DMA((2,)),
            DMA((2,)),
            DMA((2, F, 2, 2)),
            DMA((F, 2, 2)),
            DMA((2,)),
            DMA((n_tp, A)),
            DMA((n_tp, A)),
            DMA((A,)),
            DMA((A, n_tp)),
            DMA((n_tp * A,)),
            DMA((chips,)),
            DMA((chips,)),
            DMA((2 * chips,)),
            DMA((2,)),
            DMA((2,)),
            DMA((1,)),
            DMA((chips, 2)),
            DMA((chips, 2)),
            DMA((chips, 2)),
            DMA((chips, 2)),
        ],
        compiler_params=pltpu.CompilerParams(
            collective_id=0, has_side_effects=True, vmem_limit_bytes=67043328
        ),
    )(
        mix_lambda,
        head_gain,
        norm_gain,
        residual,
        by_head(query_first),
        by_head(key_first),
        by_head(value_first),
        by_map(query_second),
        by_map(key_second),
        by_head(value_second),
        out_weight.reshape(-1, width),
        up_weight,
        down_weight,
    )


def solution(mesh):
    return jax.shard_map(
        functools.partial(local, n_sp=mesh.shape["sp"], n_tp=mesh.shape["tp"]),
        mesh=mesh,
        in_specs=(
            P("sp", "tp", None),
            P("sp", "tp", None),
            P("sp", "tp", None),
            P("sp", "tp", None),
            P("sp", "tp", None),
            P("sp", "tp", None),
            P(None, "tp"),
            P(None, "tp", None),
            P(None, "tp", None, None),
            P(("sp", "tp"), None),
            P(),
            P("sp", "tp"),
            P("tp", "sp"),
        ),
        out_specs=P(("sp", "tp"), None),
        check_vma=False,
    )
```

```python
import functools
import math

import jax
import jax.numpy as jnp
from jax import lax
from jax.experimental import pallas as pl
from jax.experimental.pallas import tpu as pltpu
from jax.sharding import PartitionSpec as P

MESH = pl.DeviceIdType.MESH
EPSILON = 1e-05
BF16 = jnp.bfloat16
F32 = jnp.float32
GROUP = 2
UP, DOWN = 0, 1
Q1, Q2, K1, K2, V1 = range(5)


def when(condition):
    return pl.when(condition)


def branches(index, count, body):
    for k in range(count):
        pl.when(index == k)(functools.partial(body, k))


def xor(left, bits):
    result, weight = 0, 1
    while bits:
        low = lax.rem(lax.div(left, weight), 2)
        result = result + weight * (1 - low if bits % 2 else low)
        bits, weight = bits // 2, weight * 2
    return result + left - lax.rem(left, weight)


def aligned(value, unit):
    return pl.multiple_of(value, unit)


def layer_norm(rows, scales):
    average = jnp.mean(rows, axis=-1, keepdims=True)
    centred = rows - average
    spread = jnp.mean(centred * centred, axis=-1, keepdims=True)
    return centred * lax.rsqrt(spread + EPSILON) * scales


def combo_order(heads):
    order = []
    for h in range(heads):
        order += [(0, h), (1, h)] if h % 2 == 0 else [(1, h), (0, h)]
    return order


class Sizes:
    def __init__(self, n_sp, n_tp, heads, tokens, value, width, sub, hidden):
        self.n_sp, self.n_tp, self.heads = n_sp, n_tp, heads
        self.combos = combo_order(heads)
        self.A = len(self.combos)
        self.B = n_sp // self.A
        self.F = n_sp // GROUP
        self.tokens, self.value = tokens, value
        self.rows = tokens // n_tp
        self.width, self.sub = width, sub
        self.hidden = hidden // GROUP
        self.chips = GROUP * n_tp // 2
        self.order = range(self.A - 1, 0, -1)


def slots(kind):
    return (Q1, K1, V1) if kind == 0 else (Q1, Q2, K1, K2, V1)


def body(
    z,
    scales,
    query_block,
    key_block,
    lam_ref,
    gain_ref,
    norm_ref,
    residual_in,
    qf,
    kf,
    vf,
    qs,
    ks,
    vs,
    ow_in,
    up_in,
    down_in,
    out_ref,
    qb,
    kb,
    vw,
    head_out,
    gathered,
    ow,
    wup,
    wdn,
    x_all,
    normed_ref,
    residual_ref,
    partial,
    s1_in,
    s2_out,
    s2_in,
    sh_in,
    qkv_send,
    qkv_recv,
    kv_send,
    kv_recv,
    local_sem,
    swap_send,
    swap_recv,
    wz_send,
    wz_recv,
    wlocal_sem,
    ow_send,
    ow_recv,
    owlocal_sem,
    o_send,
    o_recv,
    x_send,
    xf_send,
    x_recv,
    xh_send,
    xh_recv,
    residual_sem,
    s1_send,
    s1_recv,
    s2_send,
    s2_recv,
    sh_send,
    sh_recv,
):
    s, t = lax.axis_index("sp"), lax.axis_index("tp")
    A, B, F, n_sp, n_tp = z.A, z.B, z.F, z.n_sp, z.n_tp
    a, b = lax.div(s, B), lax.rem(s, B)
    f, g = lax.div(s, GROUP), lax.rem(s, GROUP)
    chip, core = g * (n_tp // 2) + lax.div(t, 2), lax.rem(t, 2)
    pair = (s, t + 1 - 2 * core)
    TD, VD, R, sub, hidden = z.tokens, z.value, z.rows, z.sub, z.hidden
    half = qb.shape[2]

    def remote(src, dst, send, recv, device):
        return pltpu.make_async_remote_copy(
            src_ref=src, dst_ref=dst, send_sem=send, recv_sem=recv, device_id=device, device_id_type=MESH
        )

    vw[:, VD:] = jnp.ones((vw.shape[0], VD), BF16)
    barrier = pltpu.get_barrier_semaphore()
    for i in range(n_sp):
        for j in range(n_tp):
            @when((s != i) | (t != j))
            def greet():
                pl.semaphore_signal(barrier, inc=1, device_id=(i, j), device_id_type=MESH)
    pl.semaphore_wait(barrier, n_sp * n_tp - 1)

    def source(i, slot):
        kind, h = z.combos[i]
        if kind == 0:
            return {Q1: qf, K1: kf, V1: vf}[slot].at[h]
        if slot == V1:
            return vs.at[h]
        return (qs if slot < K1 else ks).at[h, slot % 2]

    def target(slot, origin, member):
        if slot < K1:
            return qb.at[slot, pl.ds(aligned(origin * TD, TD), TD), :]
        row = pl.ds(aligned((origin * B + member) * TD, TD), TD)
        if slot < V1:
            return kb.at[slot - K1, row, :]
        return vw.at[row, pl.ds(0, VD)]

    def qkv(me, i, slot):
        return remote(
            source(i, slot), target(slot, me, b), qkv_send.at[i, slot], qkv_recv.at[me, slot], (i * B + b, t)
        )

    def qkv_arrival(origin, slot):
        place = target(slot, origin, b)
        return remote(place, place, qkv_send.at[0, slot], qkv_recv.at[origin, slot], (s, t))

    def qkv_local(me, slot):
        return pltpu.make_async_copy(source(me, slot), target(slot, me, b), local_sem.at[slot])

    def kv(me, origin, other, slot):
        src = source(me, slot) if origin == me else target(slot, origin, b)
        return remote(
            src, target(slot, origin, b), kv_send.at[origin, other, slot - K1], kv_recv.at[origin, b, slot - K1],
            (me * B + other, t),
        )

    def kv_arrival(origin, member, slot):
        place = target(slot, origin, member)
        return remote(place, place, kv_send.at[0, 0, 0], kv_recv.at[origin, member, slot - K1], (s, t))

    def peers(count, mine, action):
        for k in range(count):
            pl.when(mine != k)(functools.partial(action, k))

    def visits(me):
        return [me] + sorted((i for i in range(A) if i != me), key=lambda i: (-abs(2 * i - A + 1), -abs(i - me)))

    def near(me):
        return sorted((i for i in range(A) if i != me), key=lambda i: abs(i - me))

    @functools.partial(branches, a, A)
    def send_heads(me):
        for i in near(me):
            for slot in slots(z.combos[i][0]):
                if slot >= K1:
                    qkv(me, i, slot).start()
        mine = slots(z.combos[me][0])

        def share(other):
            for slot in mine:
                if slot >= K1:
                    kv(me, me, other, slot).start()

        peers(B, b, share)
        for slot in mine:
            qkv_local(me, slot).start()

    def wplace(kind, block):
        if kind == UP:
            return wup.at[pl.ds(aligned(block * sub, sub), sub), :]
        return wdn.at[lax.div(block, GROUP), :, pl.ds(aligned(lax.rem(block, GROUP) * sub, sub), sub)]

    def wsource(kind, half):
        window = pl.ds(aligned(half * hidden, hidden), hidden)
        return up_in.at[:, window] if kind == UP else down_in.at[window, :]

    def swap(kind):
        return remote(
            wsource(kind, 1 - g), wplace(kind, s), swap_send.at[kind], swap_recv.at[kind], (f * GROUP + 1 - g, t)
        )

    def swap_arrival(kind):
        place = wplace(kind, f * GROUP + 1 - g)
        return remote(place, place, swap_send.at[kind], swap_recv.at[kind], (s, t))

    def wlocal(kind):
        return pltpu.make_async_copy(wsource(kind, g), wplace(kind, s), wlocal_sem.at[kind])

    def along(me, origin, index, kind, direction, raw=False):
        j = g if index == 0 else 1 - g
        place = wplace(kind, origin * GROUP + j)
        src = wsource(kind, g) if raw else place
        return remote(
            src, place, wz_send.at[(direction + 1) // 2, origin, index, kind], wz_recv.at[origin, index, kind],
            ((me + direction) * GROUP + g, t),
        )

    def crossing(me, direction):
        return (me < F // 2) != (me + direction < F // 2)

    def send_own(index, kind, crossings=(False, True)):
        @functools.partial(branches, f, F)
        def send(me):
            for direction in (1, -1):
                if 0 <= me + direction < F and crossing(me, direction) in crossings:
                    along(me, me, index, kind, direction, raw=index == 0).start()

    def relay(moves, ways=("in", "out"), forward=True):
        if not moves:
            return

        @functools.partial(branches, f, F)
        def pass_on(me):
            for k, index, kind in moves:
                for direction in (1, -1):
                    origin = me - direction * k
                    way = "out" if direction == (1 if me >= F // 2 else -1) else "in"
                    onward = 0 <= me + direction < F
                    if 0 <= origin < F and way in ways and onward == forward:
                        along(me, origin, index, kind, direction).wait_recv()
                        if onward:
                            along(me, origin, index, kind, direction).start()

    def settle(low, high, kind):
        relay(chunks(low, high, kind), forward=False)

    def chunks(low, high, kind):
        return [(k, index, kind) for k in range(low, high) for index in range(2)]

    ups = chunks(1, F - 1, UP)
    downs, downs_near, downs_far = chunks(1, F - 1, DOWN), chunks(1, F // 2, DOWN), chunks(F // 2, F - 1, DOWN)

    for kind in (UP, DOWN):
        send_own(0, kind, (False,))
        wlocal(kind).start()
    pltpu.make_async_copy(residual_in, residual_ref, residual_sem.at[0]).start()

    def ow_rows(i):
        kind, h = z.combos[i]
        return ow_in.at[pl.ds((kind * z.heads + h) * VD, VD), :]

    def ow_place(owner, i):
        return ow.at[pl.ds(aligned((owner * A + i) * VD, VD), VD), :]

    def ow_copy(i, other):
        return remote(ow_rows(i), ow_place(t, i), ow_send.at[other, i], ow_recv.at[t, i], (s, other))

    def ow_local(i):
        return pltpu.make_async_copy(ow_rows(i), ow_place(t, i), owlocal_sem.at[i])

    def ow_arrival(owner, i):
        place = ow_place(owner, i)
        return remote(place, place, ow_send.at[0, 0], ow_recv.at[owner, i], (s, t))

    for i in range(A):
        ow_local(i).start()
    peers(n_tp, t, lambda other: [ow_copy(i, other).start() for i in range(A)] and None)

    @functools.partial(branches, a, A)
    def receive_heads(me):
        mine = slots(z.combos[me][0])
        for origin in near(me):
            for slot in mine:
                if slot >= K1:
                    qkv_arrival(origin, slot).wait_recv()

            def share(other):
                for slot in mine:
                    if slot >= K1:
                        kv(me, origin, other, slot).start()

            peers(B, b, share)

    @functools.partial(branches, a, A)
    def send_queries(me):
        for i in sorted(near(me), key=lambda i: visits(i).index(me)):
            for slot in slots(z.combos[i][0]):
                if slot < K1:
                    qkv(me, i, slot).start()

    for kind in (UP, DOWN):
        swap(kind).start()
    send_own(0, UP, (True,))

    @functools.partial(branches, a, A)
    def receive_rest(me):
        mine = slots(z.combos[me][0])
        for slot in mine:
            qkv_local(me, slot).wait()
            if slot >= K1:
                for origin in range(A):
                    peers(B, b, lambda other: kv_arrival(origin, other, slot).wait_recv())

    second = sum(jnp.where(a == i, kind, 0) for i, (kind, h) in enumerate(z.combos))

    def queries_of(origin):
        @when(origin != a)
        def arrive():
            qkv_arrival(origin, Q1).wait_recv()
            pl.when(second == 1)(lambda: qkv_arrival(origin, Q2).wait_recv())

        @when(second == 0)
        def split_maps():
            low = lax.broadcasted_iota(jnp.int32, (TD, half), 1) < half // 2
            rows = pl.ds(aligned(origin * TD, TD), TD)
            queries = qb[0, rows, :]
            empty = jnp.zeros_like(queries)
            qb[1, rows, :] = jnp.where(low, empty, queries)
            qb[0, rows, :] = jnp.where(low, queries, empty)

    factor = jnp.where(second == 0, scales[0], scales[1]) * math.log2(math.e)
    lam = sum(jnp.where(a == i, lam_ref[kind, h], 0.0) for i, (kind, h) in enumerate(z.combos))
    gain = sum(jnp.where(a == i, gain_ref[kind, h : h + 1, :], 0.0) for i, (kind, h) in enumerate(z.combos))

    def attend(row):
        maxima, sums = [None, None], [None, None]
        window = pl.ds(aligned(row, query_block), query_block)
        for start in range(0, n_sp * TD, key_block):
            for c in range(2):
                scores = lax.dot_general(
                    qb[c, window, :],
                    kb[second * c, start : start + key_block, :],
                    (((1,), (1,)), ((), ())),
                    preferred_element_type=F32,
                )
                newest = jnp.max(scores, axis=-1, keepdims=True)
                if start:
                    newest = jnp.maximum(maxima[c], newest)
                weights = jnp.exp2((scores - newest) * factor).astype(BF16)
                summed = jnp.dot(weights, vw[start : start + key_block, :], preferred_element_type=F32)
                if start:
                    summed = summed + sums[c] * jnp.exp2((maxima[c] - newest) * factor)
                maxima[c], sums[c] = newest, summed
        one, two = (member[:, :VD] / member[:, VD:] for member in sums)
        attended = one - lam * two
        mean_square = jnp.mean(attended * attended, axis=-1, keepdims=True)
        head_out[window, :] = (attended * lax.rsqrt(mean_square + EPSILON) * gain).astype(BF16)

    def outs(n, owner, other):
        rows = pl.ds(aligned(owner * TD + other * R, R), R)
        return remote(
            head_out.at[rows, :], gathered.at[t * A + a], o_send.at[n, other], o_recv.at[t * A + a],
            (owner * B + b, other),
        )

    def outs_arrival(index):
        place = gathered.at[index]
        return remote(place, place, o_send.at[0, 0], o_recv.at[index], (s, t))

    blocks = TD // query_block

    def own_up():
        swap_arrival(UP).wait_recv()
        send_own(1, UP)

    def own_down():
        swap_arrival(DOWN).wait_recv()
        send_own(1, DOWN, (False,))

    plan = {2: own_up, 3: own_down}
    for point, move in zip((4, 6), ups):
        plan[point] = functools.partial(relay, [move])
    def attention_step(n, carry):
        owner = sum(
            jnp.where((a == me) & (n == k), i, 0) for me in range(A) for k, i in enumerate(visits(me))
        )
        queries_of(owner)

        def inner(m, unused):
            attend(owner * TD + m * query_block)
            for point, action in plan.items():
                if point < A * blocks:
                    pl.when(n * blocks + m == point)(action)
            return unused

        lax.fori_loop(0, blocks, inner, 0)
        for other in range(n_tp):
            @when((n > 0) | (t != other))
            def send():
                outs(n, owner, other).start()
        return carry

    lax.fori_loop(0, A, attention_step, 0)
    gathered[t * A + a] = head_out[pl.ds(aligned(a * TD + t * R, R), R), :]
    for point, action in plan.items():
        if point >= A * blocks:
            action()
    send_own(0, DOWN, (True,))
    send_own(1, DOWN, (True,))
    relay(downs, ("in",))
    relay(ups[2:3])
    pltpu.make_async_copy(residual_in, residual_ref, residual_sem.at[0]).wait()

    for i in range(A):
        ow_local(i).wait()
    for owner in range(n_tp):
        @when(t != owner)
        def weights_arrive():
            for i in range(A):
                ow_arrival(owner, i).wait_recv()
    for index in range(n_tp * A):
        pl.when((t != index // A) | (a != index % A))(lambda: outs_arrival(index).wait_recv())

    left = jnp.concatenate([gathered[index] for index in range(n_tp * A)], axis=1)
    projected = jnp.dot(left, ow[...], preferred_element_type=F32) + residual_ref[...].astype(F32)
    normed = layer_norm(projected, norm_ref[0:1, :])
    normed_ref[...] = normed
    x_all[chip * 2 + core] = normed.astype(BF16)

    def chip_at(n):
        return xor(chip, n)

    def device_of(index, c):
        return (f * GROUP + lax.div(index, n_tp // 2), lax.rem(index, n_tp // 2) * 2 + c)

    def rows_to_chip(n):
        place = x_all.at[chip * 2 + core]
        return remote(place, place, x_send.at[n], x_recv.at[chip * 2 + core], device_of(chip_at(n), core))

    def rows_to_pair(n):
        index = chip_at(n) * 2 + core
        return remote(x_all.at[index], x_all.at[index], xf_send.at[n], x_recv.at[index], pair)

    def rows_arrival(index):
        place = x_all.at[index]
        return remote(place, place, x_send.at[0], x_recv.at[index], (s, t))

    def half_rows(n, part, index):
        place = x_all.at[index, pl.ds(part * (R // 2), R // 2), :]
        return remote(place, place, xh_send.at[part], xh_recv.at[part], device_of(chip_at(n), core))

    square = z.chips == 4
    rows_to_pair(0).start()
    for n in range(1, 3 if square else z.chips):
        rows_to_chip(n).start()
    relay(ups[3:4])

    def rows_from_chip(n):
        index = chip_at(n) * 2 + core
        if square and n == 3:
            for part in range(2):
                half_rows(3, part, index).wait_recv()
        else:
            rows_arrival(index).wait_recv()
        if square and n < 3:
            half_rows(3 - n, n - 1, index).start()
        rows_to_pair(n).start()

    for n in range(1, 3 if square else z.chips):
        rows_from_chip(n)
        relay(downs_near[:1] if n == 1 else downs_near[1:] if n == 2 else [], ("out",))
    relay(ups[4:])
    settle(1, F, UP)
    for kind in (UP, DOWN):
        wlocal(kind).wait()

    def expand(n):
        index = chip_at(n)
        rows_arrival(index * 2 + 1 - core).wait_recv()
        rows = x_all[pl.ds(index * 2, 2)].reshape(2 * R, x_all.shape[2])
        expanded = jnp.dot(rows, wup[...], preferred_element_type=F32)
        ow[n * 2 * R : (n + 1) * 2 * R, :hidden] = jnp.square(jnp.maximum(expanded, 0.0)).astype(BF16)

    for n in range(z.chips):
        if square and n == 3:
            rows_from_chip(3)
        expand(n)
        relay(downs_far[:1] if n == 0 else downs_far[1:] if n == 1 else [], ("out",))

    orders = [sorted(range(F), key=lambda i: (F * ((i < F // 2) != (me < F // 2)) + abs(i - me))) for me in range(F)]
    origins = [sum(jnp.where(f == me, orders[me][m], 0) for me in range(F)) for m in range(F)]
    limits = (0, F // 2, F - 1, F)
    parts = [range(low, high) for low, high in zip(limits, limits[1:]) if low < high]

    def window(part):
        return pl.ds(parts[part][0], len(parts[part]))

    def half_to_pair(n, part):
        return remote(
            partial.at[n, 1 - core, window(part)], s1_in.at[n, window(part)], s1_send.at[n, part],
            s1_recv.at[n, part], pair,
        )

    def sum_to_chip(n, part):
        return remote(
            s2_out.at[n, window(part)], s2_in.at[n, window(part)], s2_send.at[n, part], s2_recv.at[n, part],
            device_of(chip_at(n), core),
        )

    def half_sum(way, part):
        return remote(
            s2_out.at[3, window(part), pl.ds((way - 1) * (R // 2), R // 2), :], sh_in.at[way, window(part)],
            sh_send.at[way, part], sh_recv.at[way, part], device_of(chip_at(way), core),
        )

    def contract(n, part):
        for m in parts[part]:
            result = jnp.dot(
                ow[n * 2 * R : (n + 1) * 2 * R, :hidden], wdn[origins[m]], preferred_element_type=F32
            ).astype(BF16)
            for c in range(2):
                partial[n, c, m] = result[c * R : (c + 1) * R]
        half_to_pair(n, part).start()

    def reduce(n, part):
        half_to_pair(n, part).wait_recv()
        way = 3 - n
        if square and n < 3:
            half_sum(way, part).wait_recv()
        for m in parts[part]:
            added = partial[n, core, m].astype(F32) + s1_in[n, m].astype(F32)
            if square and n < 3:
                passing = sh_in[way, m].astype(F32)
                empty = jnp.zeros_like(passing)
                added += jnp.concatenate([passing, empty] if way == 1 else [empty, passing])
            s2_out[n, m] = added.astype(BF16)
        if square and n == 3:
            for other in (1, 2):
                half_sum(other, part).start()
        else:
            sum_to_chip(n, part).start()

    order = list(range(z.chips - 1, -1, -1))
    for part in range(len(parts)):
        settle(max(1, parts[part][0]), parts[part][-1] + 1, DOWN)
        for step, n in enumerate(order):
            contract(n, part)
            if step == 1:
                reduce(order[0], part)
        for n in order[1:-1]:
            reduce(n, part)

    senders = range(1, 3 if square else z.chips)
    for part in range(len(parts)):
        half_to_pair(0, part).wait_recv()
        for n in senders:
            sum_to_chip(n, part).wait_recv()
        for m in parts[part]:
            columns = pl.ds(aligned(origins[m] * GROUP * sub, GROUP * sub), GROUP * sub)
            total = normed_ref[:, columns] + partial[0, core, m].astype(F32) + s1_in[0, m].astype(F32)
            for n in senders:
                total = total + s2_in[n, m].astype(F32)
            normed_ref[:, columns] = total
    out_ref[...] = layer_norm(normed_ref[...], norm_ref[1:2, :]).astype(BF16)

    @functools.partial(branches, a, A)
    def drain_heads(me):
        for i in near(me):
            for slot in slots(z.combos[i][0]):
                qkv(me, i, slot).wait_send()

        def drain(other):
            for slot in slots(z.combos[me][0]):
                if slot >= K1:
                    for origin in range(A):
                        kv(me, origin, other, slot).wait_send()

        peers(B, b, drain)

    for kind in (UP, DOWN):
        swap(kind).wait_send()

    @functools.partial(branches, f, F)
    def drain_weights(me):
        for direction in (1, -1):
            if 0 <= me + direction < F:
                for k in range(F):
                    origin = me - direction * k
                    if 0 <= origin < F:
                        for index in range(2):
                            for kind in (UP, DOWN):
                                along(me, origin, index, kind, direction).wait_send()

    peers(n_tp, t, lambda other: [ow_copy(i, other).wait_send() for i in range(A)] and None)
    for n in range(A):
        for other in range(n_tp):
            if n:
                outs(n, a, other).wait_send()
            else:
                pl.when(t != other)(lambda: outs(n, a, other).wait_send())
    for n in range(z.chips):
        rows_to_pair(n).wait_send()
        for part in range(len(parts)):
            half_to_pair(n, part).wait_send()
            if n in senders:
                sum_to_chip(n, part).wait_send()
        if n and not (square and n == 3):
            rows_to_chip(n).wait_send()
    if square:
        for n in (1, 2):
            half_rows(3 - n, n - 1, chip_at(n) * 2 + core).wait_send()
            for part in range(len(parts)):
                half_sum(n, part).wait_send()


def local(
    query_first,
    key_first,
    value_first,
    query_second,
    key_second,
    value_second,
    mix_lambda,
    head_gain,
    out_weight,
    residual,
    norm_gain,
    up_weight,
    down_weight,
    n_sp,
    n_tp,
):
    tokens, heads, width_first = query_first.shape
    width_second = query_second.shape[2]
    value = value_first.shape[2]
    width, hidden = up_weight.shape[0] * n_sp, up_weight.shape[1]
    sub = up_weight.shape[0]
    z = Sizes(n_sp, n_tp, heads, tokens, value, width, sub, hidden)
    half = width_second // 2

    def by_head(array):
        return array.transpose(1, 0, 2)

    def by_map(array):
        return array.reshape(tokens, heads, 2, half).transpose(1, 2, 0, 3)

    query_block = next(k for k in (384, 256, 128, tokens) if tokens % k == 0)
    key_block = next(k for k in (1024, 512, 256, tokens) if (n_sp * tokens) % k == 0)
    kernel = functools.partial(
        body, z, (1.0 / math.sqrt(width_first // 2), 1.0 / math.sqrt(half)), query_block, key_block
    )
    total = n_sp * tokens
    rows, A, B, F, chips = z.rows, z.A, z.B, z.F, z.chips
    DMA = pltpu.SemaphoreType.DMA
    vmem = pl.BlockSpec(memory_space=pltpu.VMEM)
    anywhere = pl.BlockSpec(memory_space=pl.ANY)
    return pl.pallas_call(
        kernel,
        in_specs=[pl.BlockSpec(memory_space=pltpu.SMEM), vmem, vmem] + [anywhere] * 10,
        out_specs=vmem,
        out_shape=jax.ShapeDtypeStruct((rows, width), BF16),
        scratch_shapes=[
            pltpu.VMEM((2, A * tokens, half), BF16),
            pltpu.VMEM((2, total, half), BF16),
            pltpu.VMEM((total, 2 * value), BF16),
            pltpu.VMEM((A * tokens, value), BF16),
            pltpu.VMEM((n_tp * A, rows, value), BF16),
            pltpu.VMEM((n_tp * A * value, width), BF16),
            pltpu.VMEM((width, z.hidden), BF16),
            pltpu.VMEM((F, z.hidden, GROUP * sub), BF16),
            pltpu.VMEM((2 * chips, rows, width), BF16),
            pltpu.VMEM((rows, width), F32),
            pltpu.VMEM((rows, width), BF16),
            pltpu.VMEM((chips, 2, F, rows, GROUP * sub), BF16),
            pltpu.VMEM((chips, F, rows, GROUP * sub), BF16),
            pltpu.VMEM((chips, F, rows, GROUP * sub), BF16),
            pltpu.VMEM((chips, F, rows, GROUP * sub), BF16),
            pltpu.VMEM((3, F, rows // 2, GROUP * sub), BF16),
            DMA((A, 5)),
            DMA((A, 5)),
            DMA((A, B, 3)),
            DMA((A, B, 3)),
            DMA((5,)),
            DMA((2,)),
            DMA((2,)),
            DMA((2, F, 2, 2)),
            DMA((F, 2, 2)),
            DMA((2,)),
            DMA((n_tp, A)),
            DMA((n_tp, A)),
            DMA((A,)),
            DMA((A, n_tp)),
            DMA((n_tp * A,)),
            DMA((chips,)),
            DMA((chips,)),
            DMA((2 * chips,)),
            DMA((2,)),
            DMA((2,)),
            DMA((1,)),
            DMA((chips, 3)),
            DMA((chips, 3)),
            DMA((chips, 3)),
            DMA((chips, 3)),
            DMA((3, 3)),
            DMA((3, 3)),
        ],
        compiler_params=pltpu.CompilerParams(
            collective_id=0, has_side_effects=True, vmem_limit_bytes=67043328
        ),
    )(
        mix_lambda,
        head_gain,
        norm_gain,
        residual,
        by_head(query_first),
        by_head(key_first),
        by_head(value_first),
        by_map(query_second),
        by_map(key_second),
        by_head(value_second),
        out_weight.reshape(-1, width),
        up_weight,
        down_weight,
    )


def solution(mesh):
    return jax.shard_map(
        functools.partial(local, n_sp=mesh.shape["sp"], n_tp=mesh.shape["tp"]),
        mesh=mesh,
        in_specs=(
            P("sp", "tp", None),
            P("sp", "tp", None),
            P("sp", "tp", None),
            P("sp", "tp", None),
            P("sp", "tp", None),
            P("sp", "tp", None),
            P(None, "tp"),
            P(None, "tp", None),
            P(None, "tp", None, None),
            P(("sp", "tp"), None),
            P(),
            P("sp", "tp"),
            P("tp", "sp"),
        ),
        out_specs=P(("sp", "tp"), None),
        check_vma=False,
    )
```

```python
import functools
import math

import jax
import jax.numpy as jnp
from jax import lax
from jax.experimental import pallas as pl
from jax.experimental.pallas import tpu as pltpu
from jax.sharding import PartitionSpec as P

MESH = pl.DeviceIdType.MESH
EPSILON = 1e-05
BF16 = jnp.bfloat16
F32 = jnp.float32
GROUP = 2
UP, DOWN = 0, 1
Q1, Q2, K1, K2, V1 = range(5)


def when(condition):
    return pl.when(condition)


def branches(index, count, body):
    for k in range(count):
        pl.when(index == k)(functools.partial(body, k))


def xor(left, bits):
    result, weight = 0, 1
    while bits:
        low = lax.rem(lax.div(left, weight), 2)
        result = result + weight * (1 - low if bits % 2 else low)
        bits, weight = bits // 2, weight * 2
    return result + left - lax.rem(left, weight)


def aligned(value, unit):
    return pl.multiple_of(value, unit)


def layer_norm(rows, scales):
    average = jnp.mean(rows, axis=-1, keepdims=True)
    centred = rows - average
    spread = jnp.mean(centred * centred, axis=-1, keepdims=True)
    return centred * lax.rsqrt(spread + EPSILON) * scales


def combo_order(heads):
    order = []
    for h in range(heads):
        order += [(0, h), (1, h)] if h % 2 == 0 else [(1, h), (0, h)]
    return order


class Sizes:
    def __init__(self, n_sp, n_tp, heads, tokens, value, width, sub, hidden):
        self.n_sp, self.n_tp, self.heads = n_sp, n_tp, heads
        self.combos = combo_order(heads)
        self.A = len(self.combos)
        self.B = n_sp // self.A
        self.F = n_sp // GROUP
        self.tokens, self.value = tokens, value
        self.rows = tokens // n_tp
        self.width, self.sub = width, sub
        self.hidden = hidden // GROUP
        self.chips = GROUP * n_tp // 2
        self.order = range(self.A - 1, 0, -1)


def slots(kind):
    return (Q1, K1, V1) if kind == 0 else (Q1, Q2, K1, K2, V1)


def body(
    z,
    scales,
    query_block,
    key_block,
    lam_ref,
    gain_ref,
    norm_ref,
    residual_in,
    qf,
    kf,
    vf,
    qs,
    ks,
    vs,
    ow_in,
    up_in,
    down_in,
    out_ref,
    qb,
    kb,
    vw,
    head_out,
    gathered,
    ow,
    wup,
    wdn,
    x_all,
    normed_ref,
    residual_ref,
    partial,
    s1_in,
    s2_out,
    s2_in,
    sh_in,
    qkv_send,
    qkv_recv,
    kv_send,
    kv_recv,
    local_sem,
    swap_send,
    swap_recv,
    wz_send,
    wz_recv,
    wlocal_sem,
    ow_send,
    ow_recv,
    owlocal_sem,
    o_send,
    o_recv,
    x_send,
    xf_send,
    x_recv,
    xh_send,
    xh_recv,
    residual_sem,
    s1_send,
    s1_recv,
    s2_send,
    s2_recv,
    sh_send,
    sh_recv,
):
    s, t = lax.axis_index("sp"), lax.axis_index("tp")
    A, B, F, n_sp, n_tp = z.A, z.B, z.F, z.n_sp, z.n_tp
    a, b = lax.div(s, B), lax.rem(s, B)
    f, g = lax.div(s, GROUP), lax.rem(s, GROUP)
    chip, core = g * (n_tp // 2) + lax.div(t, 2), lax.rem(t, 2)
    pair = (s, t + 1 - 2 * core)
    TD, VD, R, sub, hidden = z.tokens, z.value, z.rows, z.sub, z.hidden
    half = qb.shape[2]

    def remote(src, dst, send, recv, device):
        return pltpu.make_async_remote_copy(
            src_ref=src, dst_ref=dst, send_sem=send, recv_sem=recv, device_id=device, device_id_type=MESH
        )

    vw[:, VD:] = jnp.ones((vw.shape[0], VD), BF16)
    barrier = pltpu.get_barrier_semaphore()
    for i in range(n_sp):
        for j in range(n_tp):
            @when((s != i) | (t != j))
            def greet():
                pl.semaphore_signal(barrier, inc=1, device_id=(i, j), device_id_type=MESH)
    pl.semaphore_wait(barrier, n_sp * n_tp - 1)

    def source(i, slot):
        kind, h = z.combos[i]
        if kind == 0:
            return {Q1: qf, K1: kf, V1: vf}[slot].at[h]
        if slot == V1:
            return vs.at[h]
        return (qs if slot < K1 else ks).at[h, slot % 2]

    def target(slot, origin, member):
        if slot < K1:
            return qb.at[slot, pl.ds(aligned(origin * TD, TD), TD), :]
        row = pl.ds(aligned((origin * B + member) * TD, TD), TD)
        if slot < V1:
            return kb.at[slot - K1, row, :]
        return vw.at[row, pl.ds(0, VD)]

    def qkv(me, i, slot):
        return remote(
            source(i, slot), target(slot, me, b), qkv_send.at[i, slot], qkv_recv.at[me, slot], (i * B + b, t)
        )

    def qkv_arrival(origin, slot):
        place = target(slot, origin, b)
        return remote(place, place, qkv_send.at[0, slot], qkv_recv.at[origin, slot], (s, t))

    def qkv_local(me, slot):
        return pltpu.make_async_copy(source(me, slot), target(slot, me, b), local_sem.at[slot])

    def kv(me, origin, other, slot):
        src = source(me, slot) if origin == me else target(slot, origin, b)
        return remote(
            src, target(slot, origin, b), kv_send.at[origin, other, slot - K1], kv_recv.at[origin, b, slot - K1],
            (me * B + other, t),
        )

    def kv_arrival(origin, member, slot):
        place = target(slot, origin, member)
        return remote(place, place, kv_send.at[0, 0, 0], kv_recv.at[origin, member, slot - K1], (s, t))

    def peers(count, mine, action):
        for k in range(count):
            pl.when(mine != k)(functools.partial(action, k))

    def visits(me):
        return [me] + sorted((i for i in range(A) if i != me), key=lambda i: (-abs(2 * i - A + 1), -abs(i - me)))

    def near(me):
        return sorted((i for i in range(A) if i != me), key=lambda i: abs(i - me))

    @functools.partial(branches, a, A)
    def send_heads(me):
        for i in near(me):
            for slot in slots(z.combos[i][0]):
                if slot >= K1:
                    qkv(me, i, slot).start()
        mine = slots(z.combos[me][0])

        def share(other):
            for slot in mine:
                if slot >= K1:
                    kv(me, me, other, slot).start()

        peers(B, b, share)
        for slot in mine:
            qkv_local(me, slot).start()

    def wplace(kind, block):
        if kind == UP:
            return wup.at[pl.ds(aligned(block * sub, sub), sub), :]
        return wdn.at[lax.div(block, GROUP), :, pl.ds(aligned(lax.rem(block, GROUP) * sub, sub), sub)]

    def wsource(kind, half):
        window = pl.ds(aligned(half * hidden, hidden), hidden)
        return up_in.at[:, window] if kind == UP else down_in.at[window, :]

    def swap(kind):
        return remote(
            wsource(kind, 1 - g), wplace(kind, s), swap_send.at[kind], swap_recv.at[kind], (f * GROUP + 1 - g, t)
        )

    def swap_arrival(kind):
        place = wplace(kind, f * GROUP + 1 - g)
        return remote(place, place, swap_send.at[kind], swap_recv.at[kind], (s, t))

    def wlocal(kind):
        return pltpu.make_async_copy(wsource(kind, g), wplace(kind, s), wlocal_sem.at[kind])

    def along(me, origin, index, kind, direction, raw=False, fixed=False):
        j = g if index == 0 else 1 - g
        if fixed:
            j, index = index, lax.rem(index + g, 2)
        place = wplace(kind, origin * GROUP + j)
        src = wsource(kind, g) if raw else place
        return remote(
            src, place, wz_send.at[(direction + 1) // 2, origin, index, kind], wz_recv.at[origin, index, kind],
            ((me + direction) * GROUP + g, t),
        )

    def crossing(me, direction):
        return (me < F // 2) != (me + direction < F // 2)

    def send_own(index, kind, crossings=(False, True), fixed=False):
        @functools.partial(branches, f, F)
        def send(me):
            for direction in (1, -1):
                if 0 <= me + direction < F and crossing(me, direction) in crossings:
                    along(me, me, index, kind, direction, index == 0 and not fixed, fixed).start()

    def relay(moves, ways=("in", "out"), forward=True):
        if not moves:
            return

        @functools.partial(branches, f, F)
        def pass_on(me):
            for k, index, kind in moves:
                for direction in (1, -1):
                    origin = me - direction * k
                    way = "out" if direction == (1 if me >= F // 2 else -1) else "in"
                    onward = 0 <= me + direction < F
                    if 0 <= origin < F and way in ways and onward == forward:
                        along(me, origin, index, kind, direction, fixed=kind == DOWN).wait_recv()
                        if onward:
                            along(me, origin, index, kind, direction, fixed=kind == DOWN).start()

    def settle(low, high, kind):
        relay(chunks(low, high, kind), forward=False)

    def chunks(low, high, kind):
        return [(k, index, kind) for k in range(low, high) for index in range(2)]

    ups = chunks(1, F - 1, UP)
    downs, downs_near, downs_far = chunks(1, F - 1, DOWN), chunks(1, F // 2, DOWN), chunks(F // 2, F - 1, DOWN)

    for kind in (UP, DOWN):
        send_own(0, kind, (False,))
        wlocal(kind).start()
    pltpu.make_async_copy(residual_in, residual_ref, residual_sem.at[0]).start()

    def ow_rows(i):
        kind, h = z.combos[i]
        return ow_in.at[pl.ds((kind * z.heads + h) * VD, VD), :]

    def ow_place(owner, i):
        return ow.at[pl.ds(aligned((owner * A + i) * VD, VD), VD), :]

    def ow_copy(i, other):
        return remote(ow_rows(i), ow_place(t, i), ow_send.at[other, i], ow_recv.at[t, i], (s, other))

    def ow_local(i):
        return pltpu.make_async_copy(ow_rows(i), ow_place(t, i), owlocal_sem.at[i])

    def ow_arrival(owner, i):
        place = ow_place(owner, i)
        return remote(place, place, ow_send.at[0, 0], ow_recv.at[owner, i], (s, t))

    for i in range(A):
        ow_local(i).start()
    peers(n_tp, t, lambda other: [ow_copy(i, other).start() for i in range(A)] and None)

    @functools.partial(branches, a, A)
    def receive_heads(me):
        mine = slots(z.combos[me][0])
        for origin in near(me):
            for slot in mine:
                if slot >= K1:
                    qkv_arrival(origin, slot).wait_recv()

            def share(other):
                for slot in mine:
                    if slot >= K1:
                        kv(me, origin, other, slot).start()

            peers(B, b, share)

    @functools.partial(branches, a, A)
    def send_queries(me):
        for i in sorted(near(me), key=lambda i: visits(i).index(me)):
            for slot in slots(z.combos[i][0]):
                if slot < K1:
                    qkv(me, i, slot).start()

    at_end = (f == 0) | (f == F - 1)

    def swap_weights():
        for kind in (UP, DOWN):
            swap(kind).start()

    pl.when(jnp.logical_not(at_end))(swap_weights)
    send_own(0, UP, (True,))

    @functools.partial(branches, a, A)
    def receive_rest(me):
        mine = slots(z.combos[me][0])
        for slot in mine:
            qkv_local(me, slot).wait()
            if slot >= K1:
                for origin in range(A):
                    peers(B, b, lambda other: kv_arrival(origin, other, slot).wait_recv())

    pl.when(at_end)(swap_weights)
    for kind in (UP, DOWN):
        wlocal(kind).wait()
    second = sum(jnp.where(a == i, kind, 0) for i, (kind, h) in enumerate(z.combos))

    def queries_of(origin):
        @when(origin != a)
        def arrive():
            qkv_arrival(origin, Q1).wait_recv()
            pl.when(second == 1)(lambda: qkv_arrival(origin, Q2).wait_recv())

        @when(second == 0)
        def split_maps():
            low = lax.broadcasted_iota(jnp.int32, (TD, half), 1) < half // 2
            rows = pl.ds(aligned(origin * TD, TD), TD)
            queries = qb[0, rows, :]
            empty = jnp.zeros_like(queries)
            qb[1, rows, :] = jnp.where(low, empty, queries)
            qb[0, rows, :] = jnp.where(low, queries, empty)

    factor = jnp.where(second == 0, scales[0], scales[1]) * math.log2(math.e)
    lam = sum(jnp.where(a == i, lam_ref[kind, h], 0.0) for i, (kind, h) in enumerate(z.combos))
    gain = sum(jnp.where(a == i, gain_ref[kind, h : h + 1, :], 0.0) for i, (kind, h) in enumerate(z.combos))

    def attend(row):
        maxima, sums = [None, None], [None, None]
        window = pl.ds(aligned(row, query_block), query_block)
        for start in range(0, n_sp * TD, key_block):
            for c in range(2):
                scores = lax.dot_general(
                    qb[c, window, :],
                    kb[second * c, start : start + key_block, :],
                    (((1,), (1,)), ((), ())),
                    preferred_element_type=F32,
                )
                newest = jnp.max(scores, axis=-1, keepdims=True)
                if start:
                    newest = jnp.maximum(maxima[c], newest)
                weights = jnp.exp2((scores - newest) * factor).astype(BF16)
                summed = jnp.dot(weights, vw[start : start + key_block, :], preferred_element_type=F32)
                if start:
                    summed = summed + sums[c] * jnp.exp2((maxima[c] - newest) * factor)
                maxima[c], sums[c] = newest, summed
        one, two = (member[:, :VD] / member[:, VD:] for member in sums)
        attended = one - lam * two
        mean_square = jnp.mean(attended * attended, axis=-1, keepdims=True)
        head_out[window, :] = (attended * lax.rsqrt(mean_square + EPSILON) * gain).astype(BF16)

    def outs(n, owner, other):
        rows = pl.ds(aligned(owner * TD + other * R, R), R)
        return remote(
            head_out.at[rows, :], gathered.at[t * A + a], o_send.at[n, other], o_recv.at[t * A + a],
            (owner * B + b, other),
        )

    def outs_arrival(index):
        place = gathered.at[index]
        return remote(place, place, o_send.at[0, 0], o_recv.at[index], (s, t))

    blocks = TD // query_block

    def own_up():
        swap_arrival(UP).wait_recv()
        send_own(1, UP)

    def own_down():
        swap_arrival(DOWN).wait_recv()
        send_own(1, DOWN, (False,))

    plan = {1: own_up, 3: own_down}
    for point, move in zip((4, 6), ups):
        plan[point] = functools.partial(relay, [move])
    def attention_step(n, carry):
        owner = sum(
            jnp.where((a == me) & (n == k), i, 0) for me in range(A) for k, i in enumerate(visits(me))
        )
        queries_of(owner)

        def inner(m, unused):
            attend(owner * TD + m * query_block)
            for point, action in plan.items():
                if point < A * blocks:
                    pl.when(n * blocks + m == point)(action)
            return unused

        lax.fori_loop(0, blocks, inner, 0)
        for other in range(n_tp):
            @when((n > 0) | (t != other))
            def send():
                outs(n, owner, other).start()
        return carry

    lax.fori_loop(0, A, attention_step, 0)
    gathered[t * A + a] = head_out[pl.ds(aligned(a * TD + t * R, R), R), :]
    for point, action in plan.items():
        if point >= A * blocks:
            action()
    send_own(0, DOWN, (True,), True)
    send_own(1, DOWN, (True,), True)
    relay(downs, ("in",))
    relay(ups[2:3])
    pltpu.make_async_copy(residual_in, residual_ref, residual_sem.at[0]).wait()

    for i in range(A):
        ow_local(i).wait()
    for owner in range(n_tp):
        @when(t != owner)
        def weights_arrive():
            for i in range(A):
                ow_arrival(owner, i).wait_recv()
    for index in range(n_tp * A):
        pl.when((t != index // A) | (a != index % A))(lambda: outs_arrival(index).wait_recv())

    left = jnp.concatenate([gathered[index] for index in range(n_tp * A)], axis=1)
    projected = jnp.dot(left, ow[...], preferred_element_type=F32) + residual_ref[...].astype(F32)
    normed = layer_norm(projected, norm_ref[0:1, :])
    normed_ref[...] = normed
    x_all[chip * 2 + core] = normed.astype(BF16)

    def chip_at(n):
        return xor(chip, n)

    def device_of(index, c):
        return (f * GROUP + lax.div(index, n_tp // 2), lax.rem(index, n_tp // 2) * 2 + c)

    def rows_to_chip(n):
        place = x_all.at[chip * 2 + core]
        return remote(place, place, x_send.at[n], x_recv.at[chip * 2 + core], device_of(chip_at(n), core))

    def rows_to_pair(n):
        index = chip_at(n) * 2 + core
        return remote(x_all.at[index], x_all.at[index], xf_send.at[n], x_recv.at[index], pair)

    def rows_arrival(index):
        place = x_all.at[index]
        return remote(place, place, x_send.at[0], x_recv.at[index], (s, t))

    def half_rows(n, part, index):
        place = x_all.at[index, pl.ds(part * (R // 2), R // 2), :]
        return remote(place, place, xh_send.at[part], xh_recv.at[part], device_of(chip_at(n), core))

    square = z.chips == 4
    rows_to_pair(0).start()
    for n in range(1, 3 if square else z.chips):
        rows_to_chip(n).start()
    relay(ups[3:4])

    def rows_from_chip(n):
        index = chip_at(n) * 2 + core
        if square and n == 3:
            for part in range(2):
                half_rows(3, part, index).wait_recv()
        else:
            rows_arrival(index).wait_recv()
        if square and n < 3:
            half_rows(3 - n, n - 1, index).start()
        rows_to_pair(n).start()

    for n in range(1, 3 if square else z.chips):
        rows_from_chip(n)
        relay(downs_near[:1] if n == 1 else downs_near[1:] if n == 2 else [], ("out",))
    relay(ups[4:])
    settle(1, F, UP)

    def expand(n):
        index = chip_at(n)
        rows_arrival(index * 2 + 1 - core).wait_recv()
        rows = x_all[pl.ds(index * 2, 2)].reshape(2 * R, x_all.shape[2])
        expanded = jnp.dot(rows, wup[...], preferred_element_type=F32)
        ow[n * 2 * R : (n + 1) * 2 * R, :hidden] = jnp.square(jnp.maximum(expanded, 0.0)).astype(BF16)

    for n in range(z.chips):
        if square and n == 3:
            rows_from_chip(3)
        expand(n)
        relay(downs_far[:1] if n == 2 else [], ("out",))

    orders = [sorted(range(F), key=lambda i: (F * ((i < F // 2) != (me < F // 2)) + abs(i - me))) for me in range(F)]
    origins = [sum(jnp.where(f == me, orders[me][m], 0) for me in range(F)) for m in range(F)]
    limits = (0, F, 2 * F - 2, 2 * F - 1, 2 * F)
    parts = [range(low, high) for low, high in zip(limits, limits[1:]) if low < high]

    def window(part):
        return pl.ds(parts[part][0], len(parts[part]))

    def half_to_pair(n, part):
        return remote(
            partial.at[n, 1 - core, window(part)], s1_in.at[n, window(part)], s1_send.at[n, part],
            s1_recv.at[n, part], pair,
        )

    def sum_to_chip(n, part):
        return remote(
            s2_out.at[n, window(part)], s2_in.at[n, window(part)], s2_send.at[n, part], s2_recv.at[n, part],
            device_of(chip_at(n), core),
        )

    def half_sum(way, part):
        return remote(
            s2_out.at[3, window(part), pl.ds((way - 1) * (R // 2), R // 2), :], sh_in.at[way, window(part)],
            sh_send.at[way, part], sh_recv.at[way, part], device_of(chip_at(way), core),
        )

    def contract(n, part):
        units = list(parts[part])
        while units:
            paired = len(units) > 1
            unit = units[0]
            columns = slice(0, 2 * sub) if paired else slice(unit % 2 * sub, (unit % 2 + 1) * sub)
            result = jnp.dot(
                ow[n * 2 * R : (n + 1) * 2 * R, :hidden], wdn[origins[unit // 2], :, columns],
                preferred_element_type=F32,
            ).astype(BF16)
            for c in range(2):
                for j in range(1 + paired):
                    partial[n, c, unit + j] = result[c * R : (c + 1) * R, j * sub : (j + 1) * sub]
            units = units[1 + paired :]
        half_to_pair(n, part).start()

    def reduce(n, part):
        half_to_pair(n, part).wait_recv()
        way = 3 - n
        if square and n < 3:
            half_sum(way, part).wait_recv()
        for m in parts[part]:
            added = partial[n, core, m].astype(F32) + s1_in[n, m].astype(F32)
            if square and n < 3:
                passing = sh_in[way, m].astype(F32)
                empty = jnp.zeros_like(passing)
                added += jnp.concatenate([passing, empty] if way == 1 else [empty, passing])
            s2_out[n, m] = added.astype(BF16)
        if square and n == 3:
            for other in (1, 2):
                half_sum(other, part).start()
        else:
            sum_to_chip(n, part).start()

    order = list(range(z.chips - 1, -1, -1))
    for part in range(len(parts)):
        last = parts[part][-1] // 2
        if len(parts[part]) > 1:
            settle(max(1, parts[part][0] // 2), last + 1, DOWN)
        else:
            relay([(last, parts[part][0] % 2, DOWN)], forward=False)
        for step, n in enumerate(order):
            contract(n, part)
            if step == 1:
                reduce(order[0], part)
                relay([] if part else downs_far[1:], ("out",))
        for n in order[1:-1]:
            reduce(n, part)

    senders = range(1, 3 if square else z.chips)
    for part in range(len(parts)):
        half_to_pair(0, part).wait_recv()
        for n in senders:
            sum_to_chip(n, part).wait_recv()
        for m in parts[part]:
            columns = pl.ds(aligned((origins[m // 2] * GROUP + m % 2) * sub, sub), sub)
            total = normed_ref[:, columns] + partial[0, core, m].astype(F32) + s1_in[0, m].astype(F32)
            for n in senders:
                total = total + s2_in[n, m].astype(F32)
            normed_ref[:, columns] = total
    out_ref[...] = layer_norm(normed_ref[...], norm_ref[1:2, :]).astype(BF16)

    @functools.partial(branches, a, A)
    def drain_heads(me):
        for i in near(me):
            for slot in slots(z.combos[i][0]):
                qkv(me, i, slot).wait_send()

        def drain(other):
            for slot in slots(z.combos[me][0]):
                if slot >= K1:
                    for origin in range(A):
                        kv(me, origin, other, slot).wait_send()

        peers(B, b, drain)

    for kind in (UP, DOWN):
        swap(kind).wait_send()

    @functools.partial(branches, f, F)
    def drain_weights(me):
        for direction in (1, -1):
            if 0 <= me + direction < F:
                for k in range(F):
                    origin = me - direction * k
                    if 0 <= origin < F:
                        for index in range(2):
                            for kind in (UP, DOWN):
                                along(me, origin, index, kind, direction).wait_send()

    peers(n_tp, t, lambda other: [ow_copy(i, other).wait_send() for i in range(A)] and None)
    for n in range(A):
        for other in range(n_tp):
            if n:
                outs(n, a, other).wait_send()
            else:
                pl.when(t != other)(lambda: outs(n, a, other).wait_send())
    for n in range(z.chips):
        rows_to_pair(n).wait_send()
        for part in range(len(parts)):
            half_to_pair(n, part).wait_send()
            if n in senders:
                sum_to_chip(n, part).wait_send()
        if n and not (square and n == 3):
            rows_to_chip(n).wait_send()
    if square:
        for n in (1, 2):
            half_rows(3 - n, n - 1, chip_at(n) * 2 + core).wait_send()
            for part in range(len(parts)):
                half_sum(n, part).wait_send()


def local(
    query_first,
    key_first,
    value_first,
    query_second,
    key_second,
    value_second,
    mix_lambda,
    head_gain,
    out_weight,
    residual,
    norm_gain,
    up_weight,
    down_weight,
    n_sp,
    n_tp,
):
    tokens, heads, width_first = query_first.shape
    width_second = query_second.shape[2]
    value = value_first.shape[2]
    width, hidden = up_weight.shape[0] * n_sp, up_weight.shape[1]
    sub = up_weight.shape[0]
    z = Sizes(n_sp, n_tp, heads, tokens, value, width, sub, hidden)
    half = width_second // 2

    def by_head(array):
        return array.transpose(1, 0, 2)

    def by_map(array):
        return array.reshape(tokens, heads, 2, half).transpose(1, 2, 0, 3)

    query_block = next(k for k in (384, 256, 128, tokens) if tokens % k == 0)
    key_block = next(k for k in (1024, 512, 256, tokens) if (n_sp * tokens) % k == 0)
    kernel = functools.partial(
        body, z, (1.0 / math.sqrt(width_first // 2), 1.0 / math.sqrt(half)), query_block, key_block
    )
    total = n_sp * tokens
    rows, A, B, F, chips = z.rows, z.A, z.B, z.F, z.chips
    DMA = pltpu.SemaphoreType.DMA
    vmem = pl.BlockSpec(memory_space=pltpu.VMEM)
    anywhere = pl.BlockSpec(memory_space=pl.ANY)
    return pl.pallas_call(
        kernel,
        in_specs=[pl.BlockSpec(memory_space=pltpu.SMEM), vmem, vmem] + [anywhere] * 10,
        out_specs=vmem,
        out_shape=jax.ShapeDtypeStruct((rows, width), BF16),
        scratch_shapes=[
            pltpu.VMEM((2, A * tokens, half), BF16),
            pltpu.VMEM((2, total, half), BF16),
            pltpu.VMEM((total, 2 * value), BF16),
            pltpu.VMEM((A * tokens, value), BF16),
            pltpu.VMEM((n_tp * A, rows, value), BF16),
            pltpu.VMEM((n_tp * A * value, width), BF16),
            pltpu.VMEM((width, z.hidden), BF16),
            pltpu.VMEM((F, z.hidden, GROUP * sub), BF16),
            pltpu.VMEM((2 * chips, rows, width), BF16),
            pltpu.VMEM((rows, width), F32),
            pltpu.VMEM((rows, width), BF16),
            pltpu.VMEM((chips, 2, n_sp, rows, sub), BF16),
            pltpu.VMEM((chips, n_sp, rows, sub), BF16),
            pltpu.VMEM((chips, n_sp, rows, sub), BF16),
            pltpu.VMEM((chips, n_sp, rows, sub), BF16),
            pltpu.VMEM((3, n_sp, rows // 2, sub), BF16),
            DMA((A, 5)),
            DMA((A, 5)),
            DMA((A, B, 3)),
            DMA((A, B, 3)),
            DMA((5,)),
            DMA((2,)),
            DMA((2,)),
            DMA((2, F, 2, 2)),
            DMA((F, 2, 2)),
            DMA((2,)),
            DMA((n_tp, A)),
            DMA((n_tp, A)),
            DMA((A,)),
            DMA((A, n_tp)),
            DMA((n_tp * A,)),
            DMA((chips,)),
            DMA((chips,)),
            DMA((2 * chips,)),
            DMA((2,)),
            DMA((2,)),
            DMA((1,)),
            DMA((chips, 4)),
            DMA((chips, 4)),
            DMA((chips, 4)),
            DMA((chips, 4)),
            DMA((3, 4)),
            DMA((3, 4)),
        ],
        compiler_params=pltpu.CompilerParams(
            collective_id=0, has_side_effects=True, vmem_limit_bytes=67043328
        ),
    )(
        mix_lambda,
        head_gain,
        norm_gain,
        residual,
        by_head(query_first),
        by_head(key_first),
        by_head(value_first),
        by_map(query_second),
        by_map(key_second),
        by_head(value_second),
        out_weight.reshape(-1, width),
        up_weight,
        down_weight,
    )


def solution(mesh):
    return jax.shard_map(
        functools.partial(local, n_sp=mesh.shape["sp"], n_tp=mesh.shape["tp"]),
        mesh=mesh,
        in_specs=(
            P("sp", "tp", None),
            P("sp", "tp", None),
            P("sp", "tp", None),
            P("sp", "tp", None),
            P("sp", "tp", None),
            P("sp", "tp", None),
            P(None, "tp"),
            P(None, "tp", None),
            P(None, "tp", None, None),
            P(("sp", "tp"), None),
            P(),
            P("sp", "tp"),
            P("tp", "sp"),
        ),
        out_specs=P(("sp", "tp"), None),
        check_vma=False,
    )
```
